32 devices in a mesh: ep: 32 (over z, y, x, core).
Axes of the slice: x: 2, y: 2, z: 4, core: 2. Of those that a mesh axis runs over, the one named last changes fastest.
Arguments:
- tokens: bfloat16 [4096, 2048], P('ep'), may hold values from -6 to 6
- norm_gain: float32 [2048], replicated, may hold values from 0.1 to 1.9
- expert_ids: int32 [4096, 4], P('ep'), may hold values from 0 to 63, as said below
- gate_weights: float32 [4096, 4], P('ep'), may hold values from 0.1 to 0.6
- expert_gate: bfloat16 [64, 2048, 512], P('ep'), may hold values from -0.125 to 0.125
- expert_up: bfloat16 [64, 2048, 512], P('ep'), may hold values from -0.125 to 0.125
- expert_down: bfloat16 [64, 512, 2048], P('ep'), may hold values from -0.25 to 0.25
- shared_gate: bfloat16 [2048, 512], P('ep'), may hold values from -0.125 to 0.125
- shared_up: bfloat16 [2048, 512], P('ep'), may hold values from -0.125 to 0.125
- shared_down: bfloat16 [512, 2048], P(None, 'ep'), may hold values from -0.25 to 0.25
Outputs:
- mixed: bfloat16 [4096, 2048], P('ep')
The draws below stay inside these ranges and needn't reach their ends.
Inputs may be any that keep to these rules, and one draw needn't show every extreme that they name: `expert_ids`: expert e belongs to device e // 2; each row names 4 experts of 4 different devices; among the rows of one device at most 24 name experts of any one device, hence at most 24 any one expert; in every aligned block of 128 rows exactly 24 rows name one and the same expert.
All inputs are finite; a program needn't handle non-finite values.
Results may differ from the reference program's by a relative error of at most 0.0067.
Values may be sent and summed in bfloat16 or wider, within the bound.
A program may use at most 128 MiB of HBM per device.

```python
import jax
import jax.numpy as jnp
from jax import lax

D = 2048
DE = 512
DS = 512
TOP_K = 4
EXP_DEV = 2
TOK_DEV = 128
EXPERTS = 64
TOKENS = 4096


def route_block(block_key):
    holders = EXPERTS // EXP_DEV
    total = TOK_DEV * TOP_K
    mean_rows = total // holders
    extra = mean_rows // 2
    key_order, key_moved, key_bits, key_rows = jax.random.split(block_key, 4)
    order = jax.random.permutation(key_order, holders).astype(jnp.int32)
    moved = jax.random.randint(key_moved, (holders // 2,), 0, extra + 1).astype(jnp.int32)
    moved = moved.at[0].set(extra)
    counts = jnp.full((holders,), mean_rows, jnp.int32)
    counts = counts.at[order[0::2]].add(moved).at[order[1::2]].add(-moved)
    ends = jnp.cumsum(counts).astype(jnp.int32)
    slots = jnp.arange(total, dtype=jnp.int32)
    slot_dev = jnp.sum((ends[None, :] <= slots[:, None]).astype(jnp.int32), axis=1).astype(jnp.int32)
    bits = jax.random.randint(key_bits, (total,), 0, EXP_DEV).astype(jnp.int32)
    bits = jnp.where(slot_dev == order[0], 0, bits).astype(jnp.int32)
    expert = (slot_dev * EXP_DEV + bits).astype(jnp.int32)
    row_perm = jax.random.permutation(key_rows, TOK_DEV).astype(jnp.int32)
    row_of = row_perm[slots % TOK_DEV]
    column = (slots // TOK_DEV).astype(jnp.int32)
    table = jnp.zeros((TOK_DEV, TOP_K), jnp.int32).at[row_of, column].set(expert)
    return table


def draw_expert_ids(key, part):
    base = jax.random.fold_in(key, 7117)
    keys = jax.random.split(base, TOKENS // TOK_DEV)
    tables = jax.vmap(route_block)(keys)
    return tables.reshape(TOKENS, TOP_K).astype(jnp.int32)


def levels(key, extent, cuts, low, high):
    gain = 1.0
    for dim, blocks in cuts:
        steps = jax.random.uniform(jax.random.fold_in(jax.random.fold_in(key, 6), dim), (blocks,), jnp.float32, low / len(cuts), high / len(cuts))
        gain = gain * jnp.repeat(jnp.exp(steps), extent[dim] // blocks).reshape((-1,) + (1,) * (len(extent) - 1 - dim))
    return gain


def bell_draw(own_key, dims, scale, bound, shards=(), held_as=jnp.bfloat16):
    result = scale * jax.random.normal(own_key, dims, jnp.float32)
    if shards:
        result = result * levels(own_key, dims, shards, -0.22, 0.18)
    return jnp.clip(result, -bound, bound).astype(held_as)


def setup_inputs(seed: int = 0) -> dict:
    splits = jax.random.split(jax.random.key(seed), 11)
    return {
        "tokens": bell_draw(splits[0], (TOKENS, D), 1.0, 6.0, ((0, 32),)),
        "norm_gain": jnp.clip(1.0 + 0.18 * jax.random.normal(splits[1], (D,), jnp.float32), 0.1, 1.9),
        "expert_ids": draw_expert_ids(jax.random.fold_in(splits[10], 71), 0),
        "gate_weights": jnp.clip(0.1 + 0.5 * jax.random.uniform(splits[3], (TOKENS, TOP_K), jnp.float32) ** levels(splits[3], (TOKENS, TOP_K), ((0, 32),), -0.2, 0.2), 0.1, 0.6),
        "expert_gate": bell_draw(splits[4], (EXPERTS, D, DE), D ** -0.5, 0.125, ((0, 32),)),
        "expert_up": bell_draw(splits[5], (EXPERTS, D, DE), D ** -0.5, 0.125, ((0, 32),)),
        "expert_down": bell_draw(splits[6], (EXPERTS, DE, D), DE ** -0.5, 0.25, ((0, 32),)),
        "shared_gate": bell_draw(splits[7], (D, DS), D ** -0.5, 0.125, ((0, 32),)),
        "shared_up": bell_draw(splits[8], (D, DS), D ** -0.5, 0.125, ((0, 32),)),
        "shared_down": bell_draw(splits[9], (DS, D), DS ** -0.5, 0.25, ((1, 32),)),
    }


EPS = 1e-06

def normalize(tokens, norm_gain):
    values = tokens.astype(jnp.float32)
    scaled = values * lax.rsqrt(lax.optimization_barrier(jnp.mean(values * values, axis=-1, keepdims=True)) + EPS)
    return (scaled * norm_gain.astype(jnp.float32)).astype(jnp.bfloat16)

def swiglu(inputs, w_gate, w_up, w_down):
    gate_val = jnp.dot(inputs, w_gate, preferred_element_type=jnp.float32)
    up_val = jnp.dot(inputs, w_up, preferred_element_type=jnp.float32)
    hidden = (jax.nn.silu(gate_val) * up_val).astype(jnp.bfloat16)
    return jnp.dot(hidden, w_down, preferred_element_type=jnp.float32)

def reference(tokens, norm_gain, expert_ids, gate_weights, expert_gate, expert_up, expert_down, shared_gate, shared_up, shared_down):
    normed = normalize(tokens, norm_gain)
    count_tok = normed.shape[0]
    width = normed.shape[1]
    assign = count_tok * TOP_K
    flat_ids = expert_ids.reshape(assign).astype(jnp.int32)
    ordering = jnp.argsort(flat_ids, stable=True).astype(jnp.int32)
    sorted_ids = flat_ids[ordering]
    sorted_tok = (ordering // TOP_K).astype(jnp.int32)
    sorted_wts = gate_weights.reshape(assign)[ordering]
    counts = jnp.bincount(flat_ids, length=EXPERTS).astype(jnp.int32)
    block_rows = 256
    padded = ((counts + block_rows - 1) // block_rows * block_rows).astype(jnp.int32)
    pad_end = jnp.cumsum(padded).astype(jnp.int32)
    pad_start = pad_end - padded
    cnt_start = (jnp.cumsum(counts).astype(jnp.int32) - counts).astype(jnp.int32)
    dest = (pad_start[sorted_ids] + jnp.arange(assign, dtype=jnp.int32) - cnt_start[sorted_ids]).astype(jnp.int32)
    blocks = -(-(assign + EXPERTS * (block_rows - 1)) // block_rows)
    total_rows = blocks * block_rows
    row_tok = jnp.full((total_rows,), count_tok, jnp.int32).at[dest].set(sorted_tok)
    row_wts = jnp.zeros((total_rows,), jnp.float32).at[dest].set(sorted_wts)
    block_expert = jnp.minimum(jnp.searchsorted(pad_end, jnp.arange(blocks, dtype=jnp.int32) * block_rows, side='right'), EXPERTS - 1).astype(jnp.int32)
    padded_x = jnp.concatenate([normed, jnp.zeros((1, width), jnp.bfloat16)], axis=0)

    def step(accum, inputs_blk):
        tok_blk, wts_blk, expert = inputs_blk
        picked = padded_x[tok_blk]
        output = swiglu(picked, expert_gate[expert], expert_up[expert], expert_down[expert]).astype(jnp.bfloat16)
        accum = accum.at[tok_blk].add(output.astype(jnp.float32) * wts_blk[:, None])
        return (accum, None)
    routed, _ = lax.scan(step, jnp.zeros((count_tok + 1, width), jnp.float32), (row_tok.reshape(blocks, block_rows), row_wts.reshape(blocks, block_rows), block_expert))
    shared = swiglu(normed, shared_gate, shared_up, shared_down)
    return (routed[:count_tok] + shared).astype(jnp.bfloat16)
```

```python
import functools

import jax
import jax.numpy as jnp
from jax import lax
from jax.experimental import pallas as pl
from jax.experimental.pallas import tpu as pltpu
from jax.sharding import PartitionSpec as P

EPS = 1e-06
GROUPS = 4
CHUNKS = 4
MESH = pl.DeviceIdType.MESH
ORDER = ((0, 1, 2, 3), (1, 2, 3, 0), (2, 1, 0, 3), (3, 2, 1, 0))
BACK = ((1, 2, 3), (3, 2, 0), (0, 1, 3), (2, 1, 0))
GOAL = ((1, 1, 2), (3, 2, 0), (0, 1, 3), (2, 2, 1))
SLOT = ((0, 2, 3), (1, 1, 0), (1, 1, 0), (0, 2, 3))


def pick(table, row, column):
    value = jnp.int32(table[0][column])
    for i in range(1, len(table)):
        value = jnp.where(row == i, jnp.int32(table[i][column]), value)
    return value


def stack_rows(rank, slots):
    slot = lax.broadcasted_iota(jnp.int32, (slots, rank.shape[1]), 0).astype(jnp.float32)
    return [rank[q : q + 1, :] == slot for q in range(rank.shape[0])]


def moe_kernel(
    plane, slots, local,
    tok_ref, gain_ref, ids_ref, wts_ref, sgate_ref, sup_ref, sdown_ref,
    gate_hbm, up_hbm, down_hbm,
    out_ref,
    gate, up, down, held, pack, packed, got, back, partial, land, route, slices, spread, hidden_s,
    w_sem, rsend, rrecv, fsend, frecv, hzsend, hzrecv, hpsend, hprecv, hcsend, hcrecv,
    zsend, zrecv, dsend, drecv, bsend, brecv, lsend, lrecv,
):
    f32, bf16 = jnp.float32, jnp.bfloat16
    me = lax.axis_index("ep")
    z, p = me // plane, me % plane
    chips, chip, core = plane // 2, p // 2, p % 2
    has_low, has_high = z > 0, z < GROUPS - 1
    middle = jnp.logical_and(has_low, has_high)
    outer = jnp.logical_not(middle)
    count_tok, width = tok_ref.shape
    top = ids_ref.shape[0]
    rows = plane * slots
    part = sgate_ref.shape[1] // GROUPS
    chunk = width // CHUNKS

    weights = [
        pltpu.make_async_copy(src, dst, w_sem.at[i])
        for i, (src, dst) in enumerate(((gate_hbm, gate), (up_hbm, up), (down_hbm, down)))
    ]
    for copy in weights:
        copy.start()

    barrier = pltpu.get_barrier_semaphore()

    def greet(device):
        pl.semaphore_signal(barrier, inc=1, device_id=(device,), device_id_type=MESH)

    for i in range(1, plane):
        greet(z * plane + (p + i) % plane)
    for j in range(1, GROUPS):
        greet((z + j) % GROUPS * plane + p)

    for g in range(GROUPS):
        for i, ref in enumerate((sgate_ref, sup_ref, sdown_ref)):
            slices[g, :, i * part : (i + 1) * part] = ref[:, g * part : (g + 1) * part]
    route[z, p, :top, :] = ids_ref[...].astype(f32)
    route[z, p, top:, :] = wts_ref[...]
    values = tok_ref[...].astype(f32)
    scaled = values * lax.rsqrt(jnp.mean(values * values, axis=-1, keepdims=True) + EPS)
    held[z] = (scaled * gain_ref[...]).astype(bf16)
    spread[z, chip, core] = slices[z]

    before = (
        lax.broadcasted_iota(jnp.int32, (count_tok, count_tok), 0)
        < lax.broadcasted_iota(jnp.int32, (count_tok, count_tok), 1)
    ).astype(bf16)

    def ranks(named):
        rank = jnp.dot(named.astype(bf16), before, preferred_element_type=f32)
        return jnp.where(named, rank, -1.0)

    def make_pack(g):
        first = (
            (lax.broadcasted_iota(jnp.int32, (plane, count_tok), 0) + z * plane) * local
        ).astype(f32)
        named = jnp.zeros((plane, count_tok), jnp.bool_)
        for k in range(top):
            ids = route[g, p, k : k + 1, :]
            named = jnp.logical_or(
                named, jnp.logical_and(ids >= first, ids < first + float(local))
            )
        blocks = stack_rows(ranks(named), slots)
        pack[g] = jnp.concatenate([b.astype(f32) for b in blocks], axis=0).astype(bf16)

    def fill(g):
        for c in range(0, width, chunk):
            columns = pl.ds(c, chunk)
            packed[g, :, :, columns] = (
                jnp.dot(pack[g], held[g, :, columns], preferred_element_type=f32)
                .astype(bf16)
                .reshape(plane, slots, chunk)
            )

    make_pack(z)
    fill(z)
    pl.semaphore_wait(barrier, plane - 1 + GROUPS - 1)

    def route_copy(j, g):
        return pltpu.make_async_remote_copy(
            src_ref=route.at[g, p], dst_ref=route.at[g, p],
            send_sem=rsend.at[j], recv_sem=rrecv.at[g],
            device_id=((z + j) % GROUPS * plane + p,), device_id_type=MESH,
        )

    def route_forward(i, q):
        return pltpu.make_async_remote_copy(
            src_ref=route.at[:, q], dst_ref=route.at[:, q],
            send_sem=fsend.at[i], recv_sem=frecv.at[q],
            device_id=(z * plane + (p + i) % plane,), device_id_type=MESH,
        )

    def slice_copy(j):
        g = (z + j) % GROUPS
        return pltpu.make_async_remote_copy(
            src_ref=slices.at[g], dst_ref=spread.at[z, chip, core],
            send_sem=hzsend.at[j], recv_sem=hzrecv.at[z],
            device_id=(g * plane + p,), device_id_type=MESH,
        )

    def slice_wait(j):
        g = (z + j) % GROUPS
        pltpu.make_async_remote_copy(
            src_ref=slices.at[g], dst_ref=spread.at[g, chip, core],
            send_sem=hzsend.at[j], recv_sem=hzrecv.at[g],
            device_id=(g * plane + p,), device_id_type=MESH,
        ).wait_recv()

    def column_copy(i, g, c):
        return pltpu.make_async_remote_copy(
            src_ref=spread.at[g, c, core], dst_ref=spread.at[g, c, core],
            send_sem=hpsend.at[i, g], recv_sem=hprecv.at[c, g],
            device_id=(z * plane + (chip + i) % chips * 2 + core,), device_id_type=MESH,
        )

    def core_copy(c):
        return pltpu.make_async_remote_copy(
            src_ref=spread.at[:, :, c], dst_ref=spread.at[:, :, c],
            send_sem=hcsend.at[0], recv_sem=hcrecv.at[0],
            device_id=(me + 1 - 2 * core,), device_id_type=MESH,
        )

    def along(src, g, direction):
        return pltpu.make_async_remote_copy(
            src_ref=src, dst_ref=held.at[g],
            send_sem=zsend.at[direction, g], recv_sem=zrecv.at[g],
            device_id=(me + (plane if direction else -plane),), device_id_type=MESH,
        )

    def arrive(g):
        along(held.at[g], g, 0).wait_recv()

        @pl.when(jnp.logical_and(g > z, has_low))
        def _():
            along(held.at[g], g, 0).start()

        @pl.when(jnp.logical_and(g < z, has_high))
        def _():
            along(held.at[g], g, 1).start()

    def dispatch_copy(g, q, i):
        return pltpu.make_async_remote_copy(
            src_ref=packed.at[g, q], dst_ref=got.at[g, p],
            send_sem=dsend.at[g, i], recv_sem=drecv.at[g, i],
            device_id=(z * plane + q,), device_id_type=MESH,
        )

    def return_copy(g, q, i, c):
        columns = pl.ds(c * chunk, chunk)
        return pltpu.make_async_remote_copy(
            src_ref=got.at[g, q, :, columns], dst_ref=back.at[g, p, :, columns],
            send_sem=bsend.at[g, i, c], recv_sem=brecv.at[g, i, c],
            device_id=(z * plane + q,), device_id_type=MESH,
        )

    def dispatch(g):
        for i in range(1, plane):
            dispatch_copy(g, (p + i) % plane, i).start()
        got[g, p] = packed[g, p]

    def give_back(g, c):
        for i in range(1, plane):
            return_copy(g, (p + i) % plane, i, c).start()

    def labels(g):
        came = jnp.zeros((plane, count_tok), jnp.bool_)
        which = jnp.zeros((plane, count_tok), f32)
        scale = jnp.zeros((plane, count_tok), f32)
        first = (me * local).astype(f32)
        for k in range(top):
            ids = route[g, :, k, :] - first
            mine = jnp.logical_and(ids >= 0.0, ids < float(local))
            came = jnp.logical_or(came, mine)
            which += jnp.where(mine, ids + 1.0, 0.0)
            scale += jnp.where(mine, route[g, :, top + k, :], 0.0)
        blocks = stack_rows(ranks(came), slots)
        label, weight = [], []
        for q, block in enumerate(blocks):
            label.append(
                jnp.sum(jnp.where(block, which[q : q + 1, :], 0.0), axis=1, keepdims=True)
            )
            weight.append(
                jnp.sum(jnp.where(block, scale[q : q + 1, :], 0.0), axis=1, keepdims=True)
            )
        return jnp.concatenate(label, axis=0) - 1.0, jnp.concatenate(weight, axis=0)

    def compute(g, send):
        label, weight = labels(g)
        for i in range(1, plane):
            dispatch_copy(g, (p + i) % plane, i).wait_recv()
        x = got[g].reshape(rows, width)
        hidden = []
        for e in range(local):
            gate_val = jnp.dot(x, gate[e], preferred_element_type=f32)
            up_val = jnp.dot(x, up[e], preferred_element_type=f32)
            value = gate_val / (1.0 + jnp.exp(-gate_val)) * up_val
            hidden.append(jnp.where(label == float(e), value, 0.0).astype(bf16))
        for c in range(CHUNKS):
            columns = pl.ds(c * chunk, chunk)
            value = jnp.zeros((rows, chunk), f32)
            for e in range(local):
                value += jnp.dot(hidden[e], down[e, :, columns], preferred_element_type=f32)
            got[g, :, :, columns] = (value * weight).astype(bf16).reshape(plane, slots, chunk)
            if send is not None:

                @pl.when(send)
                def _():
                    give_back(g, c)

        back[g, p] = got[g, p]

    def combined(g, c):
        columns = pl.ds(c * chunk, chunk)
        for i in range(1, plane):
            return_copy(g, (p + i) % plane, i, c).wait_recv()
        total = lax.dot_general(
            pack[g], back[g, :, :, columns].reshape(rows, chunk), (((0,), (0,)), ((), ())),
            preferred_element_type=f32,
        )
        blocks = chunk // sgate_ref.shape[0]
        first = c * blocks
        down_t = spread[:, :, :, :, 2 * part :].reshape(width, part)[first * sgate_ref.shape[0] :][
            :chunk
        ]
        return total + lax.dot_general(
            hidden_s[g], down_t, (((1,), (1,)), ((), ())), preferred_element_type=f32
        )

    def land_copy(k, slot, goal, g, c):
        columns = pl.ds(c * chunk, chunk)
        return pltpu.make_async_remote_copy(
            src_ref=partial.at[g, :, columns], dst_ref=land.at[slot, :, columns],
            send_sem=lsend.at[k, c], recv_sem=lrecv.at[slot, c],
            device_id=(goal * plane + p,), device_id_type=MESH,
        )

    def pass_on(k):
        g = pick(BACK, z, k)
        slot, goal = pick(SLOT, z, k), pick(GOAL, z, k)
        for c in range(CHUNKS):
            columns = pl.ds(c * chunk, chunk)
            total = combined(g, c)
            if k:

                @pl.when(middle)
                def _():
                    land_copy(k, jnp.int32(k + 1), goal, g, c).wait_recv()
                    partial[g, :, columns] = (
                        total + land[k + 1, :, columns].astype(f32)
                    ).astype(bf16)

                @pl.when(outer)
                def _():
                    partial[g, :, columns] = total.astype(bf16)
            else:
                partial[g, :, columns] = total.astype(bf16)
            land_copy(k, slot, goal, g, c).start()

    for j in range(1, GROUPS):
        route_copy(j, z).start()
    for j in range(1, GROUPS):
        slice_copy(j).start()

    @pl.when(has_low)
    def _():
        along(held.at[z], z, 0).start()

    @pl.when(has_high)
    def _():
        along(held.at[z], z, 1).start()

    for i in range(1, chips):
        column_copy(i, z, chip).start()
    dispatch(z)
    for j in range(1, GROUPS):
        route_copy(j, (z + j) % GROUPS).wait_recv()
    for i in range(1, plane):
        route_forward(i, p).start()
    for j in range(1, GROUPS):
        slice_wait(j)
    for i in range(1, chips):
        for j in range(1, GROUPS):
            column_copy(i, (z + j) % GROUPS, chip).start()
    for j in range(1, GROUPS):
        make_pack((z + j) % GROUPS)

    one, two, three = (pick(ORDER, z, k) for k in range(1, GROUPS))
    arrive(one)

    @pl.when(middle)
    def _():
        arrive(three)

    fill(one)
    dispatch(one)
    for i in range(1, plane):
        route_forward(i, (p + i) % plane).wait_recv()
    for copy in weights:
        copy.wait()
    compute(z, None)
    arrive(two)
    fill(two)
    dispatch(two)
    compute(one, outer)

    @pl.when(outer)
    def _():
        arrive(three)

    fill(three)
    dispatch(three)
    for i in range(1, chips):
        for g in range(GROUPS):
            column_copy(i, g, (chip + i) % chips).wait_recv()
    core_copy(core).start()
    compute(two, jnp.logical_or(middle, outer))

    @pl.when(middle)
    def _():
        for c in range(CHUNKS):
            give_back(one, c)

    core_copy(1 - core).wait_recv()
    pre = jnp.dot(
        held[...].reshape(GROUPS * count_tok, width),
        spread[:, :, :, :, : 2 * part].reshape(width, 2 * part),
        preferred_element_type=f32,
    )
    gate_val, up_val = pre[:, :part], pre[:, part:]
    hidden_s[...] = (
        (gate_val / (1.0 + jnp.exp(-gate_val)) * up_val)
        .astype(bf16)
        .reshape(GROUPS, count_tok, part)
    )

    pass_on(0)
    compute(three, jnp.logical_or(middle, outer))
    for c in range(CHUNKS):
        give_back(z, c)
    pass_on(1)
    pass_on(2)
    for c in range(CHUNKS):
        columns = pl.ds(c * chunk, chunk)
        total = combined(z, c)
        for slot in range(2):
            land_copy(0, jnp.int32(slot), z, z, c).wait_recv()
            total += land[slot, :, columns].astype(f32)
        out_ref[:, columns] = total.astype(out_ref.dtype)

    for j in range(1, GROUPS):
        route_copy(j, z).wait_send()
        slice_copy(j).wait_send()
    for i in range(1, plane):
        route_forward(i, p).wait_send()
    for i in range(1, chips):
        for g in range(GROUPS):
            column_copy(i, g, chip).wait_send()
    core_copy(core).wait_send()
    for g in range(GROUPS):
        for i in range(1, plane):
            q = (p + i) % plane
            dispatch_copy(g, q, i).wait_send()
            for c in range(CHUNKS):
                return_copy(g, q, i, c).wait_send()

        @pl.when(jnp.logical_and(g >= z, has_low))
        def _():
            along(held.at[g], g, 0).wait_send()

        @pl.when(jnp.logical_and(g <= z, has_high))
        def _():
            along(held.at[g], g, 1).wait_send()

    for k in range(GROUPS - 1):
        for c in range(CHUNKS):
            land_copy(k, pick(SLOT, z, k), pick(GOAL, z, k), pick(BACK, z, k), c).wait_send()


def per_device(
    tokens, norm_gain, expert_ids, gate_weights, expert_gate, expert_up, expert_down,
    shared_gate, shared_up, shared_down,
):
    bf16, f32 = jnp.bfloat16, jnp.float32
    count_tok, width = tokens.shape
    top = expert_ids.shape[1]
    local = expert_gate.shape[0]
    devices = lax.axis_size("ep")
    plane = devices // GROUPS
    mean_rows = count_tok * top // devices
    capacity = mean_rows + mean_rows // 2
    slots = -(-capacity // 8) * 8
    rows = plane * slots
    depth, hidden = shared_gate.shape
    part = hidden // GROUPS
    dma = pltpu.SemaphoreType.DMA
    vmem = pl.BlockSpec(memory_space=pltpu.VMEM)
    hbm = pl.BlockSpec(memory_space=pl.ANY)
    blocks = (GROUPS, plane, slots, width)
    whole = (GROUPS, count_tok, width)
    return pl.pallas_call(
        functools.partial(moe_kernel, plane, slots, local),
        out_shape=jax.ShapeDtypeStruct((count_tok, width), bf16),
        in_specs=[vmem] * 7 + [hbm] * 3,
        out_specs=vmem,
        scratch_shapes=[
            pltpu.VMEM(expert_gate.shape, bf16),
            pltpu.VMEM(expert_up.shape, bf16),
            pltpu.VMEM(expert_down.shape, bf16),
            pltpu.VMEM(whole, bf16),
            pltpu.VMEM((GROUPS, rows, count_tok), bf16),
            pltpu.VMEM(blocks, bf16),
            pltpu.VMEM(blocks, bf16),
            pltpu.VMEM(blocks, bf16),
            pltpu.VMEM(whole, bf16),
            pltpu.VMEM(whole, bf16),
            pltpu.VMEM((GROUPS, plane, 2 * top, count_tok), f32),
            pltpu.VMEM((GROUPS, depth, 3 * part), bf16),
            pltpu.VMEM((GROUPS, plane // 2, 2, depth, 3 * part), bf16),
            pltpu.VMEM((GROUPS, count_tok, part), bf16),
            dma((3,)),
            dma((GROUPS,)),
            dma((GROUPS,)),
            dma((plane,)),
            dma((plane,)),
            dma((GROUPS,)),
            dma((GROUPS,)),
            dma((plane // 2, GROUPS)),
            dma((plane // 2, GROUPS)),
            dma((1,)),
            dma((1,)),
            dma((2, GROUPS)),
            dma((GROUPS,)),
            dma((GROUPS, plane)),
            dma((GROUPS, plane)),
            dma((GROUPS, plane, CHUNKS)),
            dma((GROUPS, plane, CHUNKS)),
            dma((GROUPS, CHUNKS)),
            dma((GROUPS, CHUNKS)),
        ],
        compiler_params=pltpu.CompilerParams(
            collective_id=0, has_side_effects=True, vmem_limit_bytes=60 * 1024 * 1024
        ),
    )(
        tokens, norm_gain.reshape(1, width), expert_ids.T, gate_weights.T,
        shared_gate, shared_up, shared_down.T, expert_gate, expert_up, expert_down,
    )


def solution(mesh):
    return jax.shard_map(
        per_device,
        mesh=mesh,
        in_specs=(
            P("ep", None),
            P(),
            P("ep", None),
            P("ep", None),
            P("ep", None, None),
            P("ep", None, None),
            P("ep", None, None),
            P("ep", None),
            P("ep", None),
            P(None, "ep"),
        ),
        out_specs=P("ep", None),
        check_vma=False,
    )
```

```python
import functools

import jax
import jax.numpy as jnp
from jax import lax
from jax.experimental import pallas as pl
from jax.experimental.pallas import tpu as pltpu
from jax.sharding import PartitionSpec as P

EPS = 1e-06
GROUPS = 4
CHUNKS = 4
MESH = pl.DeviceIdType.MESH
ORDER = ((0, 1, 2, 3), (1, 2, 3, 0), (2, 1, 0, 3), (3, 2, 1, 0))
BACK = ((2, 3, 1), (3, 0, 2), (0, 3, 1), (1, 0, 2))
GOAL = ((1, 2, 1), (3, 0, 2), (0, 3, 1), (2, 1, 2))
SLOT = ((2, 3, 0), (1, 0, 1), (1, 0, 1), (2, 3, 0))


def pick(table, row, column):
    value = jnp.int32(table[0][column])
    for i in range(1, len(table)):
        value = jnp.where(row == i, jnp.int32(table[i][column]), value)
    return value


def stack_rows(rank, slots):
    slot = lax.broadcasted_iota(jnp.int32, (slots, rank.shape[1]), 0).astype(jnp.float32)
    return [rank[q : q + 1, :] == slot for q in range(rank.shape[0])]


def moe_kernel(
    plane, slots, local,
    tok_ref, gain_ref, ids_ref, wts_ref, sgate_ref, sup_ref, sdown_ref,
    gate_hbm, up_hbm, down_hbm,
    out_ref,
    gate, up, down, held, pack, packed, got, back, partial, land, route, slices, spread,
    w_sem, rsend, rrecv, fsend, frecv, hzsend, hzrecv, hpsend, hprecv, hcsend, hcrecv,
    zsend, zrecv, dsend, drecv, bsend, brecv, lsend, lrecv,
):
    f32, bf16 = jnp.float32, jnp.bfloat16
    me = lax.axis_index("ep")
    z, p = me // plane, me % plane
    chips, chip, core = plane // 2, p // 2, p % 2
    has_low, has_high = z > 0, z < GROUPS - 1
    middle = jnp.logical_and(has_low, has_high)
    outer = jnp.logical_not(middle)
    count_tok, width = tok_ref.shape
    top = ids_ref.shape[0]
    rows = plane * slots
    part = sgate_ref.shape[1] // GROUPS
    chunk = width // CHUNKS

    weights = [
        pltpu.make_async_copy(src, dst, w_sem.at[i])
        for i, (src, dst) in enumerate(((gate_hbm, gate), (up_hbm, up), (down_hbm, down)))
    ]
    for copy in weights:
        copy.start()

    barrier = pltpu.get_barrier_semaphore()

    def greet(device):
        pl.semaphore_signal(barrier, inc=1, device_id=(device,), device_id_type=MESH)

    for i in range(1, plane):
        greet(z * plane + (p + i) % plane)
    for j in range(1, GROUPS):
        greet((z + j) % GROUPS * plane + p)

    for g in range(GROUPS):
        for i, ref in enumerate((sgate_ref, sup_ref, sdown_ref)):
            slices[g, :, i * part : (i + 1) * part] = ref[:, g * part : (g + 1) * part]
    route[z, p, :top, :] = ids_ref[...].astype(f32)
    route[z, p, top:, :] = wts_ref[...]
    values = tok_ref[...].astype(f32)
    scaled = values * lax.rsqrt(jnp.mean(values * values, axis=-1, keepdims=True) + EPS)
    held[z] = (scaled * gain_ref[...]).astype(bf16)
    spread[z, chip, core] = slices[z]

    before = (
        lax.broadcasted_iota(jnp.int32, (count_tok, count_tok), 0)
        < lax.broadcasted_iota(jnp.int32, (count_tok, count_tok), 1)
    ).astype(bf16)

    def ranks(named):
        rank = jnp.dot(named.astype(bf16), before, preferred_element_type=f32)
        return jnp.where(named, rank, -1.0)

    def make_pack(g):
        first = (
            (lax.broadcasted_iota(jnp.int32, (plane, count_tok), 0) + z * plane) * local
        ).astype(f32)
        named = jnp.zeros((plane, count_tok), jnp.bool_)
        for k in range(top):
            ids = route[g, p, k : k + 1, :]
            named = jnp.logical_or(
                named, jnp.logical_and(ids >= first, ids < first + float(local))
            )
        blocks = stack_rows(ranks(named), slots)
        pack[g] = jnp.concatenate([b.astype(f32) for b in blocks], axis=0).astype(bf16)

    def fill(g, c):
        columns = pl.ds(c * chunk, chunk)
        packed[g, :, :, columns] = (
            jnp.dot(pack[g], held[g, :, columns], preferred_element_type=f32)
            .astype(bf16)
            .reshape(plane, slots, chunk)
        )

    make_pack(z)
    for c in range(CHUNKS):
        fill(z, c)
    pl.semaphore_wait(barrier, plane - 1 + GROUPS - 1)

    def total(sem, block):
        return pltpu.make_async_copy(block, block, sem).wait()

    others = pl.ds(0, plane - 1)

    def route_copy(j, g):
        return pltpu.make_async_remote_copy(
            src_ref=route.at[g, p], dst_ref=route.at[g, p],
            send_sem=rsend.at[0], recv_sem=rrecv.at[0],
            device_id=((z + j) % GROUPS * plane + p,), device_id_type=MESH,
        )

    def route_forward(i, q):
        return pltpu.make_async_remote_copy(
            src_ref=route.at[:, q], dst_ref=route.at[:, q],
            send_sem=fsend.at[0], recv_sem=frecv.at[0],
            device_id=(z * plane + (p + i) % plane,), device_id_type=MESH,
        )

    def slice_copy(j):
        g = (z + j) % GROUPS
        return pltpu.make_async_remote_copy(
            src_ref=slices.at[g], dst_ref=spread.at[z, chip, core],
            send_sem=hzsend.at[0], recv_sem=hzrecv.at[0],
            device_id=(g * plane + p,), device_id_type=MESH,
        )

    def column_copy(i, g, c):
        return pltpu.make_async_remote_copy(
            src_ref=spread.at[g, c, core], dst_ref=spread.at[g, c, core],
            send_sem=hpsend.at[0], recv_sem=hprecv.at[0],
            device_id=(z * plane + (chip + i) % chips * 2 + core,), device_id_type=MESH,
        )

    def core_copy(c):
        return pltpu.make_async_remote_copy(
            src_ref=spread.at[:, :, c], dst_ref=spread.at[:, :, c],
            send_sem=hcsend.at[0], recv_sem=hcrecv.at[0],
            device_id=(me + 1 - 2 * core,), device_id_type=MESH,
        )

    def along(g, c, direction):
        block = held.at[g, :, pl.ds(c * chunk, chunk)]
        return pltpu.make_async_remote_copy(
            src_ref=block, dst_ref=block,
            send_sem=zsend.at[direction, g], recv_sem=zrecv.at[g, c],
            device_id=(me + (plane if direction else -plane),), device_id_type=MESH,
        )

    def arrive_chunk(g, c):
        along(g, c, 0).wait_recv()

        @pl.when(jnp.logical_and(g > z, has_low))
        def _():
            along(g, c, 0).start()

        @pl.when(jnp.logical_and(g < z, has_high))
        def _():
            along(g, c, 1).start()

    def arrive(g):
        for c in range(CHUNKS):
            arrive_chunk(g, c)

    def dispatch_copy(g, q, c):
        columns = pl.ds(c * chunk, chunk)
        return pltpu.make_async_remote_copy(
            src_ref=packed.at[g, q, :, columns], dst_ref=got.at[g, p, :, columns],
            send_sem=dsend.at[0], recv_sem=drecv.at[g],
            device_id=(z * plane + q,), device_id_type=MESH,
        )

    def return_copy(g, q, c):
        columns = pl.ds(c * chunk, chunk)
        return pltpu.make_async_remote_copy(
            src_ref=got.at[g, q, :, columns], dst_ref=back.at[g, p, :, columns],
            send_sem=bsend.at[0], recv_sem=brecv.at[g, c],
            device_id=(z * plane + q,), device_id_type=MESH,
        )

    def dispatch(g, c):
        for i in range(1, plane):
            dispatch_copy(g, (p + i) % plane, c).start()
        columns = pl.ds(c * chunk, chunk)
        got[g, p, :, columns] = packed[g, p, :, columns]

    def give_back(g, c):
        for i in range(1, plane):
            return_copy(g, (p + i) % plane, c).start()

    def labels(g):
        came = jnp.zeros((plane, count_tok), jnp.bool_)
        which = jnp.zeros((plane, count_tok), f32)
        scale = jnp.zeros((plane, count_tok), f32)
        first = (me * local).astype(f32)
        for k in range(top):
            ids = route[g, :, k, :] - first
            mine = jnp.logical_and(ids >= 0.0, ids < float(local))
            came = jnp.logical_or(came, mine)
            which += jnp.where(mine, ids + 1.0, 0.0)
            scale += jnp.where(mine, route[g, :, top + k, :], 0.0)
        blocks = stack_rows(ranks(came), slots)
        label, weight = [], []
        for q, block in enumerate(blocks):
            label.append(
                jnp.sum(jnp.where(block, which[q : q + 1, :], 0.0), axis=1, keepdims=True)
            )
            weight.append(
                jnp.sum(jnp.where(block, scale[q : q + 1, :], 0.0), axis=1, keepdims=True)
            )
        return jnp.concatenate(label, axis=0) - 1.0, jnp.concatenate(weight, axis=0)

    def compute(g, send):
        label, weight = labels(g)
        total(drecv.at[g], got.at[g, others])
        x = got[g].reshape(rows, width)
        hidden = []
        for e in range(local):
            gate_val = jnp.dot(x, gate[e], preferred_element_type=f32)
            up_val = jnp.dot(x, up[e], preferred_element_type=f32)
            value = gate_val / (1.0 + jnp.exp(-gate_val)) * up_val
            hidden.append(jnp.where(label == float(e), value, 0.0).astype(bf16))
        for c in range(CHUNKS):
            columns = pl.ds(c * chunk, chunk)
            value = jnp.zeros((rows, chunk), f32)
            for e in range(local):
                value += jnp.dot(hidden[e], down[e, :, columns], preferred_element_type=f32)
            got[g, :, :, columns] = (value * weight).astype(bf16).reshape(plane, slots, chunk)
            if send:
                give_back(g, c)

        back[g, p] = got[g, p]

    def shared_hidden(g):
        pre = jnp.dot(
            held[g], spread[:, :, :, :, : 2 * part].reshape(width, 2 * part),
            preferred_element_type=f32,
        )
        gate_val, up_val = pre[:, :part], pre[:, part:]
        return (gate_val / (1.0 + jnp.exp(-gate_val)) * up_val).astype(bf16)

    def combined(g, c, hidden):
        columns = pl.ds(c * chunk, chunk)
        total(brecv.at[g, c], back.at[g, others, :, columns])
        value = lax.dot_general(
            pack[g], back[g, :, :, columns].reshape(rows, chunk), (((0,), (0,)), ((), ())),
            preferred_element_type=f32,
        )
        blocks = chunk // sgate_ref.shape[0]
        first = c * blocks
        down_t = spread[:, :, :, :, 2 * part :].reshape(width, part)[first * sgate_ref.shape[0] :][
            :chunk
        ]
        return value + lax.dot_general(
            hidden, down_t, (((1,), (1,)), ((), ())), preferred_element_type=f32
        )

    def land_copy(k, slot, goal, g, c):
        columns = pl.ds(c * chunk, chunk)
        return pltpu.make_async_remote_copy(
            src_ref=partial.at[g, :, columns], dst_ref=land.at[slot, :, columns],
            send_sem=lsend.at[0], recv_sem=lrecv.at[slot, c],
            device_id=(goal * plane + p,), device_id_type=MESH,
        )

    def pass_on(sums):
        hidden = [shared_hidden(pick(BACK, z, k)) for k, _ in sums]
        for c in range(CHUNKS):
            columns = pl.ds(c * chunk, chunk)
            for i, (k, joined) in enumerate(sums):
                g = pick(BACK, z, k)
                slot, goal = pick(SLOT, z, k), pick(GOAL, z, k)
                value = combined(g, c, hidden[i])
                if joined:
                    extra = GROUPS - k
                    land_copy(k, jnp.int32(extra), goal, g, c).wait_recv()
                    value += land[extra, :, columns].astype(f32)
                partial[g, :, columns] = value.astype(bf16)
                land_copy(k, slot, goal, g, c).start()

    for j in range(1, GROUPS):
        route_copy(j, z).start()
    for c in range(CHUNKS):

        @pl.when(has_low)
        def _():
            along(z, c, 0).start()

        @pl.when(has_high)
        def _():
            along(z, c, 1).start()

    for j in range(1, GROUPS):
        slice_copy(j).start()
    for i in range(1, chips):
        column_copy(i, z, chip).start()
    for c in range(CHUNKS):
        dispatch(z, c)
    total(rrecv.at[0], route.at[pl.ds(0, GROUPS - 1), p])
    for i in range(1, plane):
        route_forward(i, p).start()
    for j in range(1, GROUPS):
        make_pack((z + j) % GROUPS)

    one, two, three = (pick(ORDER, z, k) for k in range(1, GROUPS))
    for c in range(CHUNKS):
        arrive_chunk(one, c)

        @pl.when(middle)
        def _():
            arrive_chunk(three, c)

        fill(one, c)
        dispatch(one, c)

    total(hzrecv.at[0], spread.at[pl.ds(0, GROUPS - 1), chip, core])
    for i in range(1, chips):
        for j in range(1, GROUPS):
            column_copy(i, (z + j) % GROUPS, chip).start()
    total(frecv.at[0], route.at[:, others])
    for copy in weights:
        copy.wait()
    compute(z, False)
    for c in range(CHUNKS):
        arrive_chunk(two, c)
        fill(two, c)
        dispatch(two, c)
    compute(one, False)
    total(hprecv.at[0], spread.at[:, pl.ds(0, chips - 1), core])
    core_copy(core).start()
    for c in range(CHUNKS):

        @pl.when(outer)
        def _():
            arrive_chunk(three, c)

        fill(three, c)
        dispatch(three, c)

    compute(two, True)
    compute(three, True)
    for c in range(CHUNKS):
        give_back(one, c)
    for c in range(CHUNKS):
        give_back(z, c)
    core_copy(1 - core).wait_recv()
    pass_on(((0, False),))

    @pl.when(outer)
    def _():
        pass_on(((1, False),))
        pass_on(((2, False),))

    @pl.when(middle)
    def _():
        pass_on(((1, True), (2, True)))

    hidden = shared_hidden(z)
    for c in range(CHUNKS):
        columns = pl.ds(c * chunk, chunk)
        value = combined(z, c, hidden)
        for slot in range(2):
            land_copy(0, jnp.int32(slot), z, z, c).wait_recv()
            value += land[slot, :, columns].astype(f32)
        out_ref[:, columns] = value.astype(out_ref.dtype)

    total(rsend.at[0], route.at[pl.ds(0, GROUPS - 1), p])
    total(hzsend.at[0], slices.at[pl.ds(0, GROUPS - 1)])
    total(fsend.at[0], route.at[:, others])
    total(hpsend.at[0], spread.at[:, pl.ds(0, chips - 1), core])
    core_copy(core).wait_send()
    total(dsend.at[0], packed.at[:, others])
    total(bsend.at[0], got.at[:, others])
    total(lsend.at[0], partial.at[pl.ds(0, GROUPS - 1)])
    for g in range(GROUPS):

        @pl.when(jnp.logical_and(g >= z, has_low))
        def _():
            total(zsend.at[0, g], held.at[g])

        @pl.when(jnp.logical_and(g <= z, has_high))
        def _():
            total(zsend.at[1, g], held.at[g])


def per_device(
    tokens, norm_gain, expert_ids, gate_weights, expert_gate, expert_up, expert_down,
    shared_gate, shared_up, shared_down,
):
    bf16, f32 = jnp.bfloat16, jnp.float32
    count_tok, width = tokens.shape
    top = expert_ids.shape[1]
    local = expert_gate.shape[0]
    devices = lax.axis_size("ep")
    plane = devices // GROUPS
    mean_rows = count_tok * top // devices
    capacity = mean_rows + mean_rows // 2
    slots = -(-capacity // 8) * 8
    rows = plane * slots
    depth, hidden = shared_gate.shape
    part = hidden // GROUPS
    dma = pltpu.SemaphoreType.DMA
    vmem = pl.BlockSpec(memory_space=pltpu.VMEM)
    hbm = pl.BlockSpec(memory_space=pl.ANY)
    blocks = (GROUPS, plane, slots, width)
    whole = (GROUPS, count_tok, width)
    return pl.pallas_call(
        functools.partial(moe_kernel, plane, slots, local),
        out_shape=jax.ShapeDtypeStruct((count_tok, width), bf16),
        in_specs=[vmem] * 7 + [hbm] * 3,
        out_specs=vmem,
        scratch_shapes=[
            pltpu.VMEM(expert_gate.shape, bf16),
            pltpu.VMEM(expert_up.shape, bf16),
            pltpu.VMEM(expert_down.shape, bf16),
            pltpu.VMEM(whole, bf16),
            pltpu.VMEM((GROUPS, rows, count_tok), bf16),
            pltpu.VMEM(blocks, bf16),
            pltpu.VMEM(blocks, bf16),
            pltpu.VMEM(blocks, bf16),
            pltpu.VMEM(whole, bf16),
            pltpu.VMEM(whole, bf16),
            pltpu.VMEM((GROUPS, plane, 2 * top, count_tok), f32),
            pltpu.VMEM((GROUPS, depth, 3 * part), bf16),
            pltpu.VMEM((GROUPS, plane // 2, 2, depth, 3 * part), bf16),
            dma((3,)),
            dma((1,)),
            dma((1,)),
            dma((1,)),
            dma((1,)),
            dma((1,)),
            dma((1,)),
            dma((1,)),
            dma((1,)),
            dma((1,)),
            dma((1,)),
            dma((2, GROUPS)),
            dma((GROUPS, CHUNKS)),
            dma((1,)),
            dma((GROUPS,)),
            dma((1,)),
            dma((GROUPS, CHUNKS)),
            dma((1,)),
            dma((GROUPS, CHUNKS)),
        ],
        compiler_params=pltpu.CompilerParams(
            collective_id=0, has_side_effects=True, vmem_limit_bytes=60 * 1024 * 1024
        ),
    )(
        tokens, norm_gain.reshape(1, width), expert_ids.T, gate_weights.T,
        shared_gate, shared_up, shared_down.T, expert_gate, expert_up, expert_down,
    )


def solution(mesh):
    return jax.shard_map(
        per_device,
        mesh=mesh,
        in_specs=(
            P("ep", None),
            P(),
            P("ep", None),
            P("ep", None),
            P("ep", None, None),
            P("ep", None, None),
            P("ep", None, None),
            P("ep", None),
            P("ep", None),
            P(None, "ep"),
        ),
        out_specs=P("ep", None),
        check_vma=False,
    )
```

```python
import functools

import jax
import jax.numpy as jnp
from jax import lax
from jax.experimental import pallas as pl
from jax.experimental.pallas import tpu as pltpu
from jax.sharding import PartitionSpec as P

EPS = 1e-06
GROUPS = 4
CHUNKS = 4
EARLY = 2
MESH = pl.DeviceIdType.MESH
ORDER = ((0, 1, 2, 3), (1, 2, 3, 0), (2, 1, 0, 3), (3, 2, 1, 0))
BACK = ((1, 2, 3), (3, 2, 0), (0, 1, 3), (2, 1, 0))
GOAL = ((1, 1, 2), (3, 2, 0), (0, 1, 3), (2, 2, 1))
SLOT = ((0, 2, 3), (1, 1, 0), (1, 1, 0), (0, 2, 3))


def pick(table, row, column):
    value = jnp.int32(table[0][column])
    for i in range(1, len(table)):
        value = jnp.where(row == i, jnp.int32(table[i][column]), value)
    return value


def stack_rows(rank, slots):
    slot = lax.broadcasted_iota(jnp.int32, (slots, rank.shape[1]), 0).astype(jnp.float32)
    return [rank[q : q + 1, :] == slot for q in range(rank.shape[0])]


def moe_kernel(
    plane, slots, local,
    tok_ref, gain_ref, ids_ref, wts_ref, sgate_ref, sup_ref, sdown_ref,
    gate_hbm, up_hbm, down_hbm,
    out_ref,
    gate, up, down, held, pack, packed, got, back, partial, land, route, slices, spread, hidden_s,
    w_sem, rsend, rrecv, fsend, frecv, hzsend, hzrecv, hpsend, hprecv, hcsend, hcrecv,
    zsend, zrecv, dsend, drecv, bsend, brecv, lsend, lrecv,
):
    f32, bf16 = jnp.float32, jnp.bfloat16
    me = lax.axis_index("ep")
    z, p = me // plane, me % plane
    chips, chip, core = plane // 2, p // 2, p % 2
    has_low, has_high = z > 0, z < GROUPS - 1
    middle = jnp.logical_and(has_low, has_high)
    outer = jnp.logical_not(middle)
    count_tok, width = tok_ref.shape
    top = ids_ref.shape[0]
    rows = plane * slots
    part = sgate_ref.shape[1] // GROUPS
    chunk = width // CHUNKS

    weights = [
        pltpu.make_async_copy(src, dst, w_sem.at[i])
        for i, (src, dst) in enumerate(((gate_hbm, gate), (up_hbm, up), (down_hbm, down)))
    ]
    for copy in weights:
        copy.start()

    barrier = pltpu.get_barrier_semaphore()

    def greet(device):
        pl.semaphore_signal(barrier, inc=1, device_id=(device,), device_id_type=MESH)

    for i in range(1, plane):
        greet(z * plane + (p + i) % plane)
    for j in range(1, GROUPS):
        greet((z + j) % GROUPS * plane + p)

    for g in range(GROUPS):
        for i, ref in enumerate((sgate_ref, sup_ref, sdown_ref)):
            slices[g, :, i * part : (i + 1) * part] = ref[:, g * part : (g + 1) * part]
    route[z, p, :top, :] = ids_ref[...].astype(f32)
    route[z, p, top:, :] = wts_ref[...]
    values = tok_ref[...].astype(f32)
    scaled = values * lax.rsqrt(jnp.mean(values * values, axis=-1, keepdims=True) + EPS)
    held[z] = (scaled * gain_ref[...]).astype(bf16)
    spread[z, chip, core] = slices[z]

    before = (
        lax.broadcasted_iota(jnp.int32, (count_tok, count_tok), 0)
        < lax.broadcasted_iota(jnp.int32, (count_tok, count_tok), 1)
    ).astype(bf16)

    def ranks(named):
        rank = jnp.dot(named.astype(bf16), before, preferred_element_type=f32)
        return jnp.where(named, rank, -1.0)

    def make_pack(g):
        first = (
            (lax.broadcasted_iota(jnp.int32, (plane, count_tok), 0) + z * plane) * local
        ).astype(f32)
        named = jnp.zeros((plane, count_tok), jnp.bool_)
        for k in range(top):
            ids = route[g, p, k : k + 1, :]
            named = jnp.logical_or(
                named, jnp.logical_and(ids >= first, ids < first + float(local))
            )
        blocks = stack_rows(ranks(named), slots)
        pack[g] = jnp.concatenate([b.astype(f32) for b in blocks], axis=0).astype(bf16)

    def fill(g, c):
        columns = pl.ds(c * chunk, chunk)
        packed[g, :, :, columns] = (
            jnp.dot(pack[g], held[g, :, columns], preferred_element_type=f32)
            .astype(bf16)
            .reshape(plane, slots, chunk)
        )

    make_pack(z)
    for c in range(CHUNKS):
        fill(z, c)
    pl.semaphore_wait(barrier, plane - 1 + GROUPS - 1)

    def total(sem, block):
        return pltpu.make_async_copy(block, block, sem).wait()

    others = pl.ds(0, plane - 1)

    def route_copy(j, g):
        return pltpu.make_async_remote_copy(
            src_ref=route.at[g, p], dst_ref=route.at[g, p],
            send_sem=rsend.at[0], recv_sem=rrecv.at[0],
            device_id=((z + j) % GROUPS * plane + p,), device_id_type=MESH,
        )

    def route_forward(i, q):
        return pltpu.make_async_remote_copy(
            src_ref=route.at[:, q], dst_ref=route.at[:, q],
            send_sem=fsend.at[0], recv_sem=frecv.at[0],
            device_id=(z * plane + (p + i) % plane,), device_id_type=MESH,
        )

    def slice_copy(j):
        g = (z + j) % GROUPS
        return pltpu.make_async_remote_copy(
            src_ref=slices.at[g], dst_ref=spread.at[z, chip, core],
            send_sem=hzsend.at[0], recv_sem=hzrecv.at[0],
            device_id=(g * plane + p,), device_id_type=MESH,
        )

    def column_copy(goal, g, c, sem):
        return pltpu.make_async_remote_copy(
            src_ref=spread.at[g, c, core], dst_ref=spread.at[g, c, core],
            send_sem=hpsend.at[0], recv_sem=hprecv.at[sem],
            device_id=(z * plane + goal * 2 + core,), device_id_type=MESH,
        )

    square = chips == 4
    beside, across = chip + 1 - 2 * (chip % 2), (chip + 2) % chips
    near = (beside, across) if square else [(chip + i) % chips for i in range(1, chips)]

    def core_copy(c):
        return pltpu.make_async_remote_copy(
            src_ref=spread.at[:, :, c], dst_ref=spread.at[:, :, c],
            send_sem=hcsend.at[0], recv_sem=hcrecv.at[0],
            device_id=(me + 1 - 2 * core,), device_id_type=MESH,
        )

    def along(g, c, direction):
        block = held.at[g, :, pl.ds(c * chunk, chunk)]
        return pltpu.make_async_remote_copy(
            src_ref=block, dst_ref=block,
            send_sem=zsend.at[direction, g], recv_sem=zrecv.at[g, c],
            device_id=(me + (plane if direction else -plane),), device_id_type=MESH,
        )

    def arrive_chunk(g, c):
        along(g, c, 0).wait_recv()

        @pl.when(jnp.logical_and(g > z, has_low))
        def _():
            along(g, c, 0).start()

        @pl.when(jnp.logical_and(g < z, has_high))
        def _():
            along(g, c, 1).start()

    def arrive(g):
        for c in range(CHUNKS):
            arrive_chunk(g, c)

    def dispatch_copy(g, q, c):
        columns = pl.ds(c * chunk, chunk)
        return pltpu.make_async_remote_copy(
            src_ref=packed.at[g, q, :, columns], dst_ref=got.at[g, p, :, columns],
            send_sem=dsend.at[0], recv_sem=drecv.at[g],
            device_id=(z * plane + q,), device_id_type=MESH,
        )

    def return_copy(g, q, c):
        columns = pl.ds(c * chunk, chunk)
        return pltpu.make_async_remote_copy(
            src_ref=got.at[g, q, :, columns], dst_ref=back.at[g, p, :, columns],
            send_sem=bsend.at[0], recv_sem=brecv.at[g, c],
            device_id=(z * plane + q,), device_id_type=MESH,
        )

    def dispatch(g, c):
        for i in range(1, plane):
            dispatch_copy(g, (p + i) % plane, c).start()
        columns = pl.ds(c * chunk, chunk)
        got[g, p, :, columns] = packed[g, p, :, columns]

    def give_back(g, c):
        for i in range(1, plane):
            return_copy(g, (p + i) % plane, c).start()

    def labels(g):
        came = jnp.zeros((plane, count_tok), jnp.bool_)
        which = jnp.zeros((plane, count_tok), f32)
        scale = jnp.zeros((plane, count_tok), f32)
        first = (me * local).astype(f32)
        for k in range(top):
            ids = route[g, :, k, :] - first
            mine = jnp.logical_and(ids >= 0.0, ids < float(local))
            came = jnp.logical_or(came, mine)
            which += jnp.where(mine, ids + 1.0, 0.0)
            scale += jnp.where(mine, route[g, :, top + k, :], 0.0)
        blocks = stack_rows(ranks(came), slots)
        label, weight = [], []
        for q, block in enumerate(blocks):
            label.append(
                jnp.sum(jnp.where(block, which[q : q + 1, :], 0.0), axis=1, keepdims=True)
            )
            weight.append(
                jnp.sum(jnp.where(block, scale[q : q + 1, :], 0.0), axis=1, keepdims=True)
            )
        return jnp.concatenate(label, axis=0) - 1.0, jnp.concatenate(weight, axis=0)

    def compute(g, send, midway=None):
        label, weight = labels(g)
        total(drecv.at[g], got.at[g, others])
        x = got[g].reshape(rows, width)
        hidden = []
        for e in range(local):
            gate_val = jnp.dot(x, gate[e], preferred_element_type=f32)
            up_val = jnp.dot(x, up[e], preferred_element_type=f32)
            value = gate_val / (1.0 + jnp.exp(-gate_val)) * up_val
            hidden.append(jnp.where(label == float(e), value, 0.0).astype(bf16))
        for c in range(CHUNKS):
            columns = pl.ds(c * chunk, chunk)
            value = jnp.zeros((rows, chunk), f32)
            for e in range(local):
                value += jnp.dot(hidden[e], down[e, :, columns], preferred_element_type=f32)
            got[g, :, :, columns] = (value * weight).astype(bf16).reshape(plane, slots, chunk)
            if send:
                give_back(g, c)
            if midway is not None and c == EARLY - 1:
                midway()

        back[g, p] = got[g, p]

    def shared_hidden(g):
        pre = jnp.dot(
            held[g], spread[:, :, :, :, : 2 * part].reshape(width, 2 * part),
            preferred_element_type=f32,
        )
        gate_val, up_val = pre[:, :part], pre[:, part:]
        hidden_s[g] = (gate_val / (1.0 + jnp.exp(-gate_val)) * up_val).astype(bf16)

    def combined(g, c):
        columns = pl.ds(c * chunk, chunk)
        total(brecv.at[g, c], back.at[g, others, :, columns])
        value = lax.dot_general(
            pack[g], back[g, :, :, columns].reshape(rows, chunk), (((0,), (0,)), ((), ())),
            preferred_element_type=f32,
        )
        blocks = chunk // sgate_ref.shape[0]
        first = c * blocks
        down_t = spread[:, :, :, :, 2 * part :].reshape(width, part)[first * sgate_ref.shape[0] :][
            :chunk
        ]
        return value + lax.dot_general(
            hidden_s[g], down_t, (((1,), (1,)), ((), ())), preferred_element_type=f32
        )

    def land_copy(k, slot, goal, g, c):
        columns = pl.ds(c * chunk, chunk)
        return pltpu.make_async_remote_copy(
            src_ref=partial.at[g, :, columns], dst_ref=land.at[slot, :, columns],
            send_sem=lsend.at[0], recv_sem=lrecv.at[slot, c],
            device_id=(goal * plane + p,), device_id_type=MESH,
        )

    def pass_on(k, c, joined=False):
        g = pick(BACK, z, k)
        columns = pl.ds(c * chunk, chunk)
        slot, goal = pick(SLOT, z, k), pick(GOAL, z, k)
        value = combined(g, c)
        if joined:
            extra = k + 1
            land_copy(k, jnp.int32(extra), goal, g, c).wait_recv()
            value += land[extra, :, columns].astype(f32)
        partial[g, :, columns] = value.astype(bf16)
        land_copy(k, slot, goal, g, c).start()

    for j in range(1, GROUPS):
        route_copy(j, z).start()
    for c in range(CHUNKS):

        @pl.when(has_low)
        def _():
            along(z, c, 0).start()

        @pl.when(has_high)
        def _():
            along(z, c, 1).start()

    for j in range(1, GROUPS):
        slice_copy(j).start()
    for goal in near:
        column_copy(goal, z, chip, 0).start()
    for c in range(CHUNKS):
        dispatch(z, c)
    total(rrecv.at[0], route.at[pl.ds(0, GROUPS - 1), p])
    for i in range(1, plane):
        route_forward(i, p).start()
    for j in range(1, GROUPS):
        make_pack((z + j) % GROUPS)

    one, two, three = (pick(ORDER, z, k) for k in range(1, GROUPS))
    for c in range(CHUNKS):
        arrive_chunk(one, c)

        @pl.when(middle)
        def _():
            arrive_chunk(three, c)

        fill(one, c)
        dispatch(one, c)

    total(hzrecv.at[0], spread.at[pl.ds(0, GROUPS - 1), chip, core])
    for goal in near:
        for j in range(1, GROUPS):
            column_copy(goal, (z + j) % GROUPS, chip, 0).start()
    total(frecv.at[0], route.at[:, others])
    for copy in weights:
        copy.wait()
    compute(z, False)

    def hand_over():
        total(hprecv.at[0], spread.at[:, pl.ds(0, len(near)), core])
        if square:
            for g in range(GROUPS // 2):
                column_copy(across, g, beside, 1).start()
            for g in range(GROUPS // 2, GROUPS):
                column_copy(beside, g, across, 1).start()

    def share():
        if square:
            total(hprecv.at[1], spread.at[:, 0, core])
        core_copy(core).start()

    for c in range(CHUNKS):
        arrive_chunk(two, c)
        fill(two, c)
        dispatch(two, c)
        if c == 1:

            @pl.when(middle)
            def _():
                hand_over()

    @pl.when(outer)
    def _():
        hand_over()

    compute(one, False)

    @pl.when(outer)
    def _():
        for c in range(EARLY):
            give_back(one, c)
        for c in range(EARLY):
            arrive_chunk(three, c)
            fill(three, c)
            dispatch(three, c)
        share()

    @pl.when(middle)
    def _():
        fill(three, 0)
        dispatch(three, 0)

    def rest_of_three():
        @pl.when(outer)
        def _():
            for c in range(EARLY, CHUNKS):
                arrive_chunk(three, c)
                fill(three, c)
                dispatch(three, c)

    compute(two, True, rest_of_three)

    @pl.when(outer)
    def _():
        core_copy(1 - core).wait_recv()
        shared_hidden(one)
        for c in range(EARLY):
            pass_on(0, c)
        shared_hidden(two)
        for c in range(EARLY):
            pass_on(1, c)

    @pl.when(middle)
    def _():
        for c in range(EARLY):
            give_back(one, c)
        for c in range(1, CHUNKS):
            fill(three, c)
            dispatch(three, c)
        for c in range(EARLY, CHUNKS):
            give_back(one, c)
        share()
        core_copy(1 - core).wait_recv()
        shared_hidden(two)
        for c in range(CHUNKS):
            pass_on(0, c)
        shared_hidden(one)
        for c in range(EARLY):
            pass_on(1, c, True)

    def third_of_two():
        @pl.when(outer)
        def _():
            pass_on(1, EARLY)

    compute(three, True, third_of_two)

    @pl.when(outer)
    def _():
        for c in range(EARLY, CHUNKS):
            give_back(one, c)

    for c in range(CHUNKS):
        give_back(z, c)

    @pl.when(outer)
    def _():
        shared_hidden(three)
        for c in range(EARLY + 1, CHUNKS):
            pass_on(1, c)
        for c in range(CHUNKS):
            pass_on(2, c)
        for c in range(EARLY, CHUNKS):
            pass_on(0, c)

    @pl.when(middle)
    def _():
        shared_hidden(three)
        for c in range(EARLY, CHUNKS):
            pass_on(1, c, True)
        for c in range(CHUNKS):
            pass_on(2, c, True)

    shared_hidden(z)
    for c in range(CHUNKS):
        columns = pl.ds(c * chunk, chunk)
        value = combined(z, c)
        for slot in range(2):
            land_copy(0, jnp.int32(slot), z, z, c).wait_recv()
            value += land[slot, :, columns].astype(f32)
        out_ref[:, columns] = value.astype(out_ref.dtype)

    total(rsend.at[0], route.at[pl.ds(0, GROUPS - 1), p])
    total(hzsend.at[0], slices.at[pl.ds(0, GROUPS - 1)])
    total(fsend.at[0], route.at[:, others])
    total(hpsend.at[0], spread.at[:, pl.ds(0, chips - 1), core])
    core_copy(core).wait_send()
    total(dsend.at[0], packed.at[:, others])
    total(bsend.at[0], got.at[:, others])
    total(lsend.at[0], partial.at[pl.ds(0, GROUPS - 1)])
    for g in range(GROUPS):

        @pl.when(jnp.logical_and(g >= z, has_low))
        def _():
            total(zsend.at[0, g], held.at[g])

        @pl.when(jnp.logical_and(g <= z, has_high))
        def _():
            total(zsend.at[1, g], held.at[g])


def per_device(
    tokens, norm_gain, expert_ids, gate_weights, expert_gate, expert_up, expert_down,
    shared_gate, shared_up, shared_down,
):
    bf16, f32 = jnp.bfloat16, jnp.float32
    count_tok, width = tokens.shape
    top = expert_ids.shape[1]
    local = expert_gate.shape[0]
    devices = lax.axis_size("ep")
    plane = devices // GROUPS
    mean_rows = count_tok * top // devices
    capacity = mean_rows + mean_rows // 2
    slots = -(-capacity // 8) * 8
    rows = plane * slots
    depth, hidden = shared_gate.shape
    part = hidden // GROUPS
    dma = pltpu.SemaphoreType.DMA
    vmem = pl.BlockSpec(memory_space=pltpu.VMEM)
    hbm = pl.BlockSpec(memory_space=pl.ANY)
    blocks = (GROUPS, plane, slots, width)
    whole = (GROUPS, count_tok, width)
    return pl.pallas_call(
        functools.partial(moe_kernel, plane, slots, local),
        out_shape=jax.ShapeDtypeStruct((count_tok, width), bf16),
        in_specs=[vmem] * 7 + [hbm] * 3,
        out_specs=vmem,
        scratch_shapes=[
            pltpu.VMEM(expert_gate.shape, bf16),
            pltpu.VMEM(expert_up.shape, bf16),
            pltpu.VMEM(expert_down.shape, bf16),
            pltpu.VMEM(whole, bf16),
            pltpu.VMEM((GROUPS, rows, count_tok), bf16),
            pltpu.VMEM(blocks, bf16),
            pltpu.VMEM(blocks, bf16),
            pltpu.VMEM(blocks, bf16),
            pltpu.VMEM(whole, bf16),
            pltpu.VMEM(whole, bf16),
            pltpu.VMEM((GROUPS, plane, 2 * top, count_tok), f32),
            pltpu.VMEM((GROUPS, depth, 3 * part), bf16),
            pltpu.VMEM((GROUPS, plane // 2, 2, depth, 3 * part), bf16),
            pltpu.VMEM((GROUPS, count_tok, part), bf16),
            dma((3,)),
            dma((1,)),
            dma((1,)),
            dma((1,)),
            dma((1,)),
            dma((1,)),
            dma((1,)),
            dma((1,)),
            dma((2,)),
            dma((1,)),
            dma((1,)),
            dma((2, GROUPS)),
            dma((GROUPS, CHUNKS)),
            dma((1,)),
            dma((GROUPS,)),
            dma((1,)),
            dma((GROUPS, CHUNKS)),
            dma((1,)),
            dma((GROUPS, CHUNKS)),
        ],
        compiler_params=pltpu.CompilerParams(
            collective_id=0, has_side_effects=True, vmem_limit_bytes=60 * 1024 * 1024
        ),
    )(
        tokens, norm_gain.reshape(1, width), expert_ids.T, gate_weights.T,
        shared_gate, shared_up, shared_down.T, expert_gate, expert_up, expert_down,
    )


def solution(mesh):
    return jax.shard_map(
        per_device,
        mesh=mesh,
        in_specs=(
            P("ep", None),
            P(),
            P("ep", None),
            P("ep", None),
            P("ep", None, None),
            P("ep", None, None),
            P("ep", None, None),
            P("ep", None),
            P("ep", None),
            P(None, "ep"),
        ),
        out_specs=P("ep", None),
        check_vma=False,
    )
```

```python
import functools

import jax
import jax.numpy as jnp
from jax import lax
from jax.experimental import pallas as pl
from jax.experimental.pallas import tpu as pltpu
from jax.sharding import PartitionSpec as P

EPS = 1e-06
GROUPS = 4
CHUNKS = 4
EARLY = 2
MESH = pl.DeviceIdType.MESH
ORDER = ((0, 1, 2, 3), (1, 2, 3, 0), (2, 1, 0, 3), (3, 2, 1, 0))
BACK = ((1, 2, 3), (3, 2, 0), (0, 1, 3), (2, 1, 0))
GOAL = ((1, 1, 2), (3, 2, 0), (0, 1, 3), (2, 2, 1))
SLOT = ((0, 2, 3), (1, 1, 0), (1, 1, 0), (0, 2, 3))


def pick(table, row, column):
    value = jnp.int32(table[0][column])
    for i in range(1, len(table)):
        value = jnp.where(row == i, jnp.int32(table[i][column]), value)
    return value


def stack_rows(rank, slots):
    slot = lax.broadcasted_iota(jnp.int32, (slots, rank.shape[1]), 0).astype(jnp.float32)
    return [rank[q : q + 1, :] == slot for q in range(rank.shape[0])]


def moe_kernel(
    plane, slots, local,
    tok_hbm, gain_hbm, ids_hbm, wts_hbm, sgate_hbm, sup_hbm, sdown_hbm,
    gate_hbm, up_hbm, down_hbm,
    out_ref,
    tok_ref, gain_ref, ids_ref, wts_ref, sgate_ref, sup_ref, sdown_ref, in_sem,
    gate, up, down, held, pack, packed, got, back, partial, land, route, slices, spread, hidden_s,
    w_sem, rsend, rrecv, fsend, frecv, hzsend, hzrecv, hpsend, hprecv, hcsend, hcrecv,
    zsend, zrecv, dsend, drecv, bsend, brecv, lsend, lrecv,
):
    f32, bf16 = jnp.float32, jnp.bfloat16
    me = lax.axis_index("ep")
    z, p = me // plane, me % plane
    chips, chip, core = plane // 2, p // 2, p % 2
    has_low, has_high = z > 0, z < GROUPS - 1
    middle = jnp.logical_and(has_low, has_high)
    outer = jnp.logical_not(middle)
    count_tok, width = tok_ref.shape
    top = ids_ref.shape[0]
    rows = plane * slots
    part = sgate_ref.shape[1] // GROUPS
    chunk = width // CHUNKS

    inputs = [
        pltpu.make_async_copy(src, dst, in_sem.at[i])
        for i, (src, dst) in enumerate(
            (
                (tok_hbm, tok_ref), (gain_hbm, gain_ref), (ids_hbm, ids_ref),
                (wts_hbm, wts_ref), (sgate_hbm, sgate_ref), (sup_hbm, sup_ref),
                (sdown_hbm, sdown_ref),
            )
        )
    ]
    for copy in inputs:
        copy.start()
    barrier = pltpu.get_barrier_semaphore()

    def greet(device):
        pl.semaphore_signal(barrier, inc=1, device_id=(device,), device_id_type=MESH)

    for i in range(1, plane):
        greet(z * plane + (p + i) % plane)
    for j in range(1, GROUPS):
        greet((z + j) % GROUPS * plane + p)

    weights = [
        pltpu.make_async_copy(src, dst, w_sem.at[i])
        for i, (src, dst) in enumerate(((gate_hbm, gate), (up_hbm, up), (down_hbm, down)))
    ]
    for copy in weights:
        copy.start()

    for copy in inputs:
        copy.wait()
    for g in range(GROUPS):
        for i, ref in enumerate((sgate_ref, sup_ref, sdown_ref)):
            slices[g, :, i * part : (i + 1) * part] = ref[:, g * part : (g + 1) * part]
    route[z, p, :top, :] = ids_ref[...].astype(f32)
    route[z, p, top:, :] = wts_ref[...]
    values = tok_ref[...].astype(f32)
    scaled = values * lax.rsqrt(jnp.mean(values * values, axis=-1, keepdims=True) + EPS)
    held[z] = (scaled * gain_ref[...]).astype(bf16)
    spread[z, chip, core] = slices[z]

    before = (
        lax.broadcasted_iota(jnp.int32, (count_tok, count_tok), 0)
        < lax.broadcasted_iota(jnp.int32, (count_tok, count_tok), 1)
    ).astype(bf16)

    def ranks(named):
        rank = jnp.dot(named.astype(bf16), before, preferred_element_type=f32)
        return jnp.where(named, rank, -1.0)

    def make_pack(g):
        first = (
            (lax.broadcasted_iota(jnp.int32, (plane, count_tok), 0) + z * plane) * local
        ).astype(f32)
        named = jnp.zeros((plane, count_tok), jnp.bool_)
        for k in range(top):
            ids = route[g, p, k : k + 1, :]
            named = jnp.logical_or(
                named, jnp.logical_and(ids >= first, ids < first + float(local))
            )
        blocks = stack_rows(ranks(named), slots)
        pack[g] = jnp.concatenate([b.astype(f32) for b in blocks], axis=0).astype(bf16)

    def fill(g, c):
        columns = pl.ds(c * chunk, chunk)
        packed[g, :, :, columns] = (
            jnp.dot(pack[g], held[g, :, columns], preferred_element_type=f32)
            .astype(bf16)
            .reshape(plane, slots, chunk)
        )

    pl.semaphore_wait(barrier, plane - 1 + GROUPS - 1)

    def total(sem, block):
        return pltpu.make_async_copy(block, block, sem).wait()

    others = pl.ds(0, plane - 1)

    def route_copy(j, g):
        return pltpu.make_async_remote_copy(
            src_ref=route.at[g, p], dst_ref=route.at[g, p],
            send_sem=rsend.at[0], recv_sem=rrecv.at[0],
            device_id=((z + j) % GROUPS * plane + p,), device_id_type=MESH,
        )

    def route_forward(i, q):
        return pltpu.make_async_remote_copy(
            src_ref=route.at[:, q], dst_ref=route.at[:, q],
            send_sem=fsend.at[0], recv_sem=frecv.at[0],
            device_id=(z * plane + (p + i) % plane,), device_id_type=MESH,
        )

    def slice_copy(j):
        g = (z + j) % GROUPS
        return pltpu.make_async_remote_copy(
            src_ref=slices.at[g], dst_ref=spread.at[z, chip, core],
            send_sem=hzsend.at[0], recv_sem=hzrecv.at[0],
            device_id=(g * plane + p,), device_id_type=MESH,
        )

    def column_copy(goal, g, c, sem):
        return pltpu.make_async_remote_copy(
            src_ref=spread.at[g, c, core], dst_ref=spread.at[g, c, core],
            send_sem=hpsend.at[0], recv_sem=hprecv.at[sem],
            device_id=(z * plane + goal * 2 + core,), device_id_type=MESH,
        )

    square = chips == 4
    beside, across = chip + 1 - 2 * (chip % 2), (chip + 2) % chips
    near = (beside, across) if square else [(chip + i) % chips for i in range(1, chips)]

    def core_copy(c):
        return pltpu.make_async_remote_copy(
            src_ref=spread.at[:, :, c], dst_ref=spread.at[:, :, c],
            send_sem=hcsend.at[0], recv_sem=hcrecv.at[0],
            device_id=(me + 1 - 2 * core,), device_id_type=MESH,
        )

    def along(g, c, direction):
        block = held.at[g, :, pl.ds(c * chunk, chunk)]
        return pltpu.make_async_remote_copy(
            src_ref=block, dst_ref=block,
            send_sem=zsend.at[direction, g], recv_sem=zrecv.at[g, c],
            device_id=(me + (plane if direction else -plane),), device_id_type=MESH,
        )

    def arrive_chunk(g, c):
        along(g, c, 0).wait_recv()

        @pl.when(jnp.logical_and(g > z, has_low))
        def _():
            along(g, c, 0).start()

        @pl.when(jnp.logical_and(g < z, has_high))
        def _():
            along(g, c, 1).start()

    def arrive(g):
        for c in range(CHUNKS):
            arrive_chunk(g, c)

    def dispatch_copy(g, q, c):
        columns = pl.ds(c * chunk, chunk)
        return pltpu.make_async_remote_copy(
            src_ref=packed.at[g, q, :, columns], dst_ref=got.at[g, p, :, columns],
            send_sem=dsend.at[0], recv_sem=drecv.at[g],
            device_id=(z * plane + q,), device_id_type=MESH,
        )

    def return_copy(g, q, c):
        columns = pl.ds(c * chunk, chunk)
        return pltpu.make_async_remote_copy(
            src_ref=got.at[g, q, :, columns], dst_ref=back.at[g, p, :, columns],
            send_sem=bsend.at[0], recv_sem=brecv.at[g, c],
            device_id=(z * plane + q,), device_id_type=MESH,
        )

    def dispatch(g, c):
        for i in range(1, plane):
            dispatch_copy(g, (p + i) % plane, c).start()
        columns = pl.ds(c * chunk, chunk)
        got[g, p, :, columns] = packed[g, p, :, columns]

    def give_back(g, c):
        for i in range(1, plane):
            return_copy(g, (p + i) % plane, c).start()

    def labels(g):
        came = jnp.zeros((plane, count_tok), jnp.bool_)
        which = jnp.zeros((plane, count_tok), f32)
        scale = jnp.zeros((plane, count_tok), f32)
        first = (me * local).astype(f32)
        for k in range(top):
            ids = route[g, :, k, :] - first
            mine = jnp.logical_and(ids >= 0.0, ids < float(local))
            came = jnp.logical_or(came, mine)
            which += jnp.where(mine, ids + 1.0, 0.0)
            scale += jnp.where(mine, route[g, :, top + k, :], 0.0)
        blocks = stack_rows(ranks(came), slots)
        label, weight = [], []
        for q, block in enumerate(blocks):
            label.append(
                jnp.sum(jnp.where(block, which[q : q + 1, :], 0.0), axis=1, keepdims=True)
            )
            weight.append(
                jnp.sum(jnp.where(block, scale[q : q + 1, :], 0.0), axis=1, keepdims=True)
            )
        return jnp.concatenate(label, axis=0) - 1.0, jnp.concatenate(weight, axis=0)

    def compute(g, send, midway=None):
        label, weight = labels(g)
        total(drecv.at[g], got.at[g, others])
        x = got[g].reshape(rows, width)
        hidden = []
        for e in range(local):
            gate_val = jnp.dot(x, gate[e], preferred_element_type=f32)
            up_val = jnp.dot(x, up[e], preferred_element_type=f32)
            value = gate_val / (1.0 + jnp.exp(-gate_val)) * up_val
            hidden.append(jnp.where(label == float(e), value, 0.0).astype(bf16))
        for c in range(CHUNKS):
            columns = pl.ds(c * chunk, chunk)
            value = jnp.zeros((rows, chunk), f32)
            for e in range(local):
                value += jnp.dot(hidden[e], down[e, :, columns], preferred_element_type=f32)
            got[g, :, :, columns] = (value * weight).astype(bf16).reshape(plane, slots, chunk)
            if send:
                give_back(g, c)
            if midway is not None and c == EARLY - 1:
                midway()

        back[g, p] = got[g, p]

    def shared_hidden(g):
        pre = jnp.dot(
            held[g], spread[:, :, :, :, : 2 * part].reshape(width, 2 * part),
            preferred_element_type=f32,
        )
        gate_val, up_val = pre[:, :part], pre[:, part:]
        hidden_s[g] = (gate_val / (1.0 + jnp.exp(-gate_val)) * up_val).astype(bf16)

    def combined(g, c):
        columns = pl.ds(c * chunk, chunk)
        total(brecv.at[g, c], back.at[g, others, :, columns])
        value = lax.dot_general(
            pack[g], back[g, :, :, columns].reshape(rows, chunk), (((0,), (0,)), ((), ())),
            preferred_element_type=f32,
        )
        blocks = chunk // sgate_ref.shape[0]
        first = c * blocks
        down_t = spread[:, :, :, :, 2 * part :].reshape(width, part)[first * sgate_ref.shape[0] :][
            :chunk
        ]
        return value + lax.dot_general(
            hidden_s[g], down_t, (((1,), (1,)), ((), ())), preferred_element_type=f32
        )

    def land_copy(k, slot, goal, g, c):
        columns = pl.ds(c * chunk, chunk)
        return pltpu.make_async_remote_copy(
            src_ref=partial.at[g, :, columns], dst_ref=land.at[slot, :, columns],
            send_sem=lsend.at[0], recv_sem=lrecv.at[slot, c],
            device_id=(goal * plane + p,), device_id_type=MESH,
        )

    def pass_on(k, c, joined=False):
        g = pick(BACK, z, k)
        columns = pl.ds(c * chunk, chunk)
        slot, goal = pick(SLOT, z, k), pick(GOAL, z, k)
        value = combined(g, c)
        if joined:
            extra = k + 1
            land_copy(k, jnp.int32(extra), goal, g, c).wait_recv()
            value += land[extra, :, columns].astype(f32)
        partial[g, :, columns] = value.astype(bf16)
        land_copy(k, slot, goal, g, c).start()

    for j in range(1, GROUPS):
        route_copy(j, z).start()
    for c in range(CHUNKS):

        @pl.when(has_low)
        def _():
            along(z, c, 0).start()

        @pl.when(has_high)
        def _():
            along(z, c, 1).start()

    for j in range(1, GROUPS):
        slice_copy(j).start()
    for goal in near:
        column_copy(goal, z, chip, 0).start()
    make_pack(z)
    for c in range(CHUNKS):
        fill(z, c)
        dispatch(z, c)
    total(rrecv.at[0], route.at[pl.ds(0, GROUPS - 1), p])
    for i in range(1, plane):
        route_forward(i, p).start()
    for j in range(1, GROUPS):
        make_pack((z + j) % GROUPS)

    one, two, three = (pick(ORDER, z, k) for k in range(1, GROUPS))
    for c in range(CHUNKS):
        arrive_chunk(one, c)

        @pl.when(middle)
        def _():
            arrive_chunk(three, c)

        fill(one, c)
        dispatch(one, c)

    total(hzrecv.at[0], spread.at[pl.ds(0, GROUPS - 1), chip, core])
    for goal in near:
        for j in range(1, GROUPS):
            column_copy(goal, (z + j) % GROUPS, chip, 0).start()
    total(frecv.at[0], route.at[:, others])
    for copy in weights:
        copy.wait()
    compute(z, False)

    def hand_over():
        total(hprecv.at[0], spread.at[:, pl.ds(0, len(near)), core])
        if square:
            for g in range(GROUPS // 2):
                column_copy(across, g, beside, 1).start()
            for g in range(GROUPS // 2, GROUPS):
                column_copy(beside, g, across, 1).start()

    def share():
        if square:
            total(hprecv.at[1], spread.at[:, 0, core])
        core_copy(core).start()

    for c in range(CHUNKS):
        arrive_chunk(two, c)
        fill(two, c)
        dispatch(two, c)
        if c == 1:

            @pl.when(middle)
            def _():
                hand_over()

    @pl.when(outer)
    def _():
        hand_over()

    compute(one, False)

    @pl.when(outer)
    def _():
        for c in range(EARLY):
            give_back(one, c)
        for c in range(EARLY):
            arrive_chunk(three, c)
            fill(three, c)
            dispatch(three, c)
        share()

    @pl.when(middle)
    def _():
        fill(three, 0)
        dispatch(three, 0)

    def rest_of_three():
        @pl.when(outer)
        def _():
            for c in range(EARLY, CHUNKS):
                arrive_chunk(three, c)
                fill(three, c)
                dispatch(three, c)

    compute(two, True, rest_of_three)

    @pl.when(outer)
    def _():
        core_copy(1 - core).wait_recv()
        shared_hidden(one)
        for c in range(EARLY):
            pass_on(0, c)
        shared_hidden(two)
        for c in range(EARLY):
            pass_on(1, c)

    @pl.when(middle)
    def _():
        for c in range(EARLY):
            give_back(one, c)
        for c in range(1, CHUNKS):
            fill(three, c)
            dispatch(three, c)
        for c in range(EARLY, CHUNKS):
            give_back(one, c)
        share()
        core_copy(1 - core).wait_recv()
        shared_hidden(two)
        for c in range(CHUNKS):
            pass_on(0, c)
        shared_hidden(one)
        for c in range(EARLY):
            pass_on(1, c, True)

    def third_of_two():
        @pl.when(outer)
        def _():
            pass_on(1, EARLY)

    compute(three, True, third_of_two)

    @pl.when(outer)
    def _():
        for c in range(EARLY, CHUNKS):
            give_back(one, c)

    for c in range(CHUNKS):
        give_back(z, c)

    @pl.when(outer)
    def _():
        shared_hidden(three)
        for c in range(EARLY + 1, CHUNKS):
            pass_on(1, c)
        for c in range(CHUNKS):
            pass_on(2, c)
        for c in range(EARLY, CHUNKS):
            pass_on(0, c)

    @pl.when(middle)
    def _():
        shared_hidden(three)
        for c in range(EARLY, CHUNKS):
            pass_on(1, c, True)
        for c in range(CHUNKS):
            pass_on(2, c, True)

    shared_hidden(z)
    for c in range(CHUNKS):
        columns = pl.ds(c * chunk, chunk)
        value = combined(z, c)
        for slot in range(2):
            land_copy(0, jnp.int32(slot), z, z, c).wait_recv()
            value += land[slot, :, columns].astype(f32)
        out_ref[:, columns] = value.astype(out_ref.dtype)

    total(rsend.at[0], route.at[pl.ds(0, GROUPS - 1), p])
    total(hzsend.at[0], slices.at[pl.ds(0, GROUPS - 1)])
    total(fsend.at[0], route.at[:, others])
    total(hpsend.at[0], spread.at[:, pl.ds(0, chips - 1), core])
    core_copy(core).wait_send()
    total(dsend.at[0], packed.at[:, others])
    total(bsend.at[0], got.at[:, others])
    total(lsend.at[0], partial.at[pl.ds(0, GROUPS - 1)])
    for g in range(GROUPS):

        @pl.when(jnp.logical_and(g >= z, has_low))
        def _():
            total(zsend.at[0, g], held.at[g])

        @pl.when(jnp.logical_and(g <= z, has_high))
        def _():
            total(zsend.at[1, g], held.at[g])


def per_device(
    tokens, norm_gain, expert_ids, gate_weights, expert_gate, expert_up, expert_down,
    shared_gate, shared_up, shared_down,
):
    bf16, f32 = jnp.bfloat16, jnp.float32
    count_tok, width = tokens.shape
    top = expert_ids.shape[1]
    local = expert_gate.shape[0]
    devices = lax.axis_size("ep")
    plane = devices // GROUPS
    mean_rows = count_tok * top // devices
    capacity = mean_rows + mean_rows // 2
    slots = -(-capacity // 8) * 8
    rows = plane * slots
    depth, hidden = shared_gate.shape
    part = hidden // GROUPS
    dma = pltpu.SemaphoreType.DMA
    hbm = pl.BlockSpec(memory_space=pltpu.HBM)
    blocks = (GROUPS, plane, slots, width)
    whole = (GROUPS, count_tok, width)
    return pl.pallas_call(
        functools.partial(moe_kernel, plane, slots, local),
        out_shape=jax.ShapeDtypeStruct((count_tok, width), bf16),
        in_specs=[hbm] * 10,
        out_specs=pl.BlockSpec(memory_space=pltpu.VMEM),
        scratch_shapes=[
            pltpu.VMEM(tokens.shape, bf16),
            pltpu.VMEM((1, width), f32),
            pltpu.VMEM((top, count_tok), jnp.int32),
            pltpu.VMEM((top, count_tok), f32),
            pltpu.VMEM(shared_gate.shape, bf16),
            pltpu.VMEM(shared_gate.shape, bf16),
            pltpu.VMEM(shared_gate.shape, bf16),
            dma((7,)),
            pltpu.VMEM(expert_gate.shape, bf16),
            pltpu.VMEM(expert_up.shape, bf16),
            pltpu.VMEM(expert_down.shape, bf16),
            pltpu.VMEM(whole, bf16),
            pltpu.VMEM((GROUPS, rows, count_tok), bf16),
            pltpu.VMEM(blocks, bf16),
            pltpu.VMEM(blocks, bf16),
            pltpu.VMEM(blocks, bf16),
            pltpu.VMEM(whole, bf16),
            pltpu.VMEM(whole, bf16),
            pltpu.VMEM((GROUPS, plane, 2 * top, count_tok), f32),
            pltpu.VMEM((GROUPS, depth, 3 * part), bf16),
            pltpu.VMEM((GROUPS, plane // 2, 2, depth, 3 * part), bf16),
            pltpu.VMEM((GROUPS, count_tok, part), bf16),
            dma((3,)),
            dma((1,)),
            dma((1,)),
            dma((1,)),
            dma((1,)),
            dma((1,)),
            dma((1,)),
            dma((1,)),
            dma((2,)),
            dma((1,)),
            dma((1,)),
            dma((2, GROUPS)),
            dma((GROUPS, CHUNKS)),
            dma((1,)),
            dma((GROUPS,)),
            dma((1,)),
            dma((GROUPS, CHUNKS)),
            dma((1,)),
            dma((GROUPS, CHUNKS)),
        ],
        compiler_params=pltpu.CompilerParams(
            collective_id=0, has_side_effects=True, vmem_limit_bytes=52 * 1024 * 1024
        ),
    )(
        *[
            pltpu.with_memory_space_constraint(x, pltpu.HBM)
            for x in (
                tokens, norm_gain.reshape(1, width), expert_ids.T, gate_weights.T,
                shared_gate, shared_up, shared_down.T, expert_gate, expert_up, expert_down,
            )
        ]
    )


def solution(mesh):
    return jax.shard_map(
        per_device,
        mesh=mesh,
        in_specs=(
            P("ep", None),
            P(),
            P("ep", None),
            P("ep", None),
            P("ep", None, None),
            P("ep", None, None),
            P("ep", None, None),
            P("ep", None),
            P("ep", None),
            P(None, "ep"),
        ),
        out_specs=P("ep", None),
        check_vma=False,
    )
```

```python
import functools

import jax
import jax.numpy as jnp
from jax import lax
from jax.experimental import pallas as pl
from jax.experimental.pallas import tpu as pltpu
from jax.sharding import PartitionSpec as P

EPS = 1e-06
GROUPS = 4
CHUNKS = 4
EARLY = 2
HALVES = 2
MESH = pl.DeviceIdType.MESH
ORDER = ((0, 1, 2, 3), (1, 2, 3, 0), (2, 1, 0, 3), (3, 2, 1, 0))
BACK = ((1, 2, 3), (3, 2, 0), (0, 1, 3), (2, 1, 0))
GOAL = ((1, 1, 2), (3, 2, 0), (0, 1, 3), (2, 2, 1))
SLOT = ((0, 2, 3), (1, 1, 0), (1, 1, 0), (0, 2, 3))


def pick(table, row, column):
    value = jnp.int32(table[0][column])
    for i in range(1, len(table)):
        value = jnp.where(row == i, jnp.int32(table[i][column]), value)
    return value


def stack_rows(rank, slots):
    slot = lax.broadcasted_iota(jnp.int32, (slots, rank.shape[1]), 0).astype(jnp.float32)
    return [rank[q : q + 1, :] == slot for q in range(rank.shape[0])]


def moe_kernel(
    plane, slots, local,
    tok_hbm, gain_hbm, ids_hbm, wts_hbm, sgate_hbm, sup_hbm, sdown_hbm,
    gate_hbm, up_hbm, down_hbm,
    out_ref,
    tok_ref, gain_ref, ids_ref, wts_ref, sgate_ref, sup_ref, sdown_ref, in_sem,
    gate, up, down, held, pack, unpack, packed, got, back, partial, land, route, share_of, slices, spread, hidden_s,
    w_sem, rsend, rrecv, fsend, frecv, hzsend, hzrecv, hpsend, hprecv, hcsend, hcrecv,
    zsend, zrecv, dsend, drecv, bsend, brecv, lsend, lrecv,
):
    f32, bf16 = jnp.float32, jnp.bfloat16
    me = lax.axis_index("ep")
    z, p = me // plane, me % plane
    chips, chip, core = plane // 2, p // 2, p % 2
    has_low, has_high = z > 0, z < GROUPS - 1
    middle = jnp.logical_and(has_low, has_high)
    outer = jnp.logical_not(middle)
    count_tok, width = tok_ref.shape
    top = ids_ref.shape[0]
    rows = plane * slots
    part = sgate_ref.shape[1] // GROUPS
    chunk = width // CHUNKS
    piece = chunk // HALVES

    inputs = [
        pltpu.make_async_copy(src, dst, in_sem.at[i])
        for i, (src, dst) in enumerate(
            (
                (tok_hbm, tok_ref), (gain_hbm, gain_ref), (ids_hbm, ids_ref),
                (wts_hbm, wts_ref), (sgate_hbm, sgate_ref), (sup_hbm, sup_ref),
                (sdown_hbm, sdown_ref),
            )
        )
    ]
    for copy in inputs:
        copy.start()
    barrier = pltpu.get_barrier_semaphore()

    def greet(device):
        pl.semaphore_signal(barrier, inc=1, device_id=(device,), device_id_type=MESH)

    for i in range(1, plane):
        greet(z * plane + (p + i) % plane)
    for j in range(1, GROUPS):
        greet((z + j) % GROUPS * plane + p)

    weights = [
        pltpu.make_async_copy(src, dst, w_sem.at[i])
        for i, (src, dst) in enumerate(((gate_hbm, gate), (up_hbm, up), (down_hbm, down)))
    ]
    for copy in weights:
        copy.start()

    for copy in inputs:
        copy.wait()
    for g in range(GROUPS):
        for i, ref in enumerate((sgate_ref, sup_ref, sdown_ref)):
            slices[g, :, i * part : (i + 1) * part] = ref[:, g * part : (g + 1) * part]
    route[p, z] = ids_ref[...].astype(f32)
    share_of[z] = wts_ref[...]
    values = tok_ref[...].astype(f32)
    scaled = values * lax.rsqrt(jnp.mean(values * values, axis=-1, keepdims=True) + EPS)
    held[z] = (scaled * gain_ref[...]).astype(bf16)
    spread[z, chip, core] = slices[z]

    before = (
        lax.broadcasted_iota(jnp.int32, (count_tok, count_tok), 0)
        < lax.broadcasted_iota(jnp.int32, (count_tok, count_tok), 1)
    ).astype(bf16)

    def ranks(named):
        rank = jnp.dot(named.astype(bf16), before, preferred_element_type=f32)
        return jnp.where(named, rank, -1.0)

    def make_pack(g):
        first = (
            (lax.broadcasted_iota(jnp.int32, (plane, count_tok), 0) + z * plane) * local
        ).astype(f32)
        named = jnp.zeros((plane, count_tok), jnp.bool_)
        scale = jnp.zeros((plane, count_tok), f32)
        for k in range(top):
            ids = route[p, g, k : k + 1, :]
            here = jnp.logical_and(ids >= first, ids < first + float(local))
            named = jnp.logical_or(named, here)
            scale += jnp.where(here, share_of[g, k : k + 1, :], 0.0)
        blocks = stack_rows(ranks(named), slots)
        pack[g] = jnp.concatenate([b.astype(f32) for b in blocks], axis=0).astype(bf16)
        weighted = jnp.concatenate(
            [jnp.where(b, scale[q : q + 1, :], 0.0) for q, b in enumerate(blocks)], axis=0
        )
        upper = weighted.astype(bf16)
        unpack[g, 0] = upper
        unpack[g, 1] = (weighted - upper.astype(f32)).astype(bf16)

    def fill(g, c):
        columns = pl.ds(c * chunk, chunk)
        packed[g, :, :, columns] = (
            jnp.dot(pack[g], held[g, :, columns], preferred_element_type=f32)
            .astype(bf16)
            .reshape(plane, slots, chunk)
        )

    pl.semaphore_wait(barrier, plane - 1 + GROUPS - 1)

    def total(sem, block):
        return pltpu.make_async_copy(block, block, sem).wait()

    others = pl.ds(0, plane - 1)

    def route_copy(j, ref, sem):
        return pltpu.make_async_remote_copy(
            src_ref=ref, dst_ref=ref,
            send_sem=rsend.at[sem], recv_sem=rrecv.at[sem],
            device_id=((z + j) % GROUPS * plane + p,), device_id_type=MESH,
        )

    def route_forward(i, q):
        return pltpu.make_async_remote_copy(
            src_ref=route.at[q], dst_ref=route.at[q],
            send_sem=fsend.at[0], recv_sem=frecv.at[0],
            device_id=(z * plane + (p + i) % plane,), device_id_type=MESH,
        )

    def slice_copy(j):
        g = (z + j) % GROUPS
        return pltpu.make_async_remote_copy(
            src_ref=slices.at[g], dst_ref=spread.at[z, chip, core],
            send_sem=hzsend.at[0], recv_sem=hzrecv.at[0],
            device_id=(g * plane + p,), device_id_type=MESH,
        )

    def column_copy(goal, g, c, sem):
        return pltpu.make_async_remote_copy(
            src_ref=spread.at[g, c, core], dst_ref=spread.at[g, c, core],
            send_sem=hpsend.at[0], recv_sem=hprecv.at[sem],
            device_id=(z * plane + goal * 2 + core,), device_id_type=MESH,
        )

    square = chips == 4
    beside, across = chip + 1 - 2 * (chip % 2), (chip + 2) % chips
    near = (beside, across) if square else [(chip + i) % chips for i in range(1, chips)]

    def core_copy(c):
        return pltpu.make_async_remote_copy(
            src_ref=spread.at[:, :, c], dst_ref=spread.at[:, :, c],
            send_sem=hcsend.at[0], recv_sem=hcrecv.at[0],
            device_id=(me + 1 - 2 * core,), device_id_type=MESH,
        )

    def along(g, c, direction):
        block = held.at[g, :, pl.ds(c * chunk, chunk)]
        return pltpu.make_async_remote_copy(
            src_ref=block, dst_ref=block,
            send_sem=zsend.at[direction, g], recv_sem=zrecv.at[g, c],
            device_id=(me + (plane if direction else -plane),), device_id_type=MESH,
        )

    def arrive_chunk(g, c):
        along(g, c, 0).wait_recv()

        @pl.when(jnp.logical_and(g > z, has_low))
        def _():
            along(g, c, 0).start()

        @pl.when(jnp.logical_and(g < z, has_high))
        def _():
            along(g, c, 1).start()

    def arrive(g):
        for c in range(CHUNKS):
            arrive_chunk(g, c)

    def dispatch_copy(g, q, c):
        columns = pl.ds(c * chunk, chunk)
        return pltpu.make_async_remote_copy(
            src_ref=packed.at[g, q, :, columns], dst_ref=got.at[g, p, :, columns],
            send_sem=dsend.at[0], recv_sem=drecv.at[g],
            device_id=(z * plane + q,), device_id_type=MESH,
        )

    def return_copy(g, q, c):
        columns = pl.ds(c * chunk, chunk)
        return pltpu.make_async_remote_copy(
            src_ref=got.at[g, q, :, columns], dst_ref=back.at[g, p, :, columns],
            send_sem=bsend.at[0], recv_sem=brecv.at[g, c],
            device_id=(z * plane + q,), device_id_type=MESH,
        )

    def dispatch(g, c):
        for i in range(1, plane):
            dispatch_copy(g, (p + i) % plane, c).start()
        columns = pl.ds(c * chunk, chunk)
        got[g, p, :, columns] = packed[g, p, :, columns]

    def give_back(g, c):
        for i in range(1, plane):
            return_copy(g, (p + i) % plane, c).start()

    def labels(g):
        came = jnp.zeros((plane, count_tok), jnp.bool_)
        which = jnp.zeros((plane, count_tok), f32)
        first = (me * local).astype(f32)
        for k in range(top):
            ids = route[:, g, k, :] - first
            mine = jnp.logical_and(ids >= 0.0, ids < float(local))
            came = jnp.logical_or(came, mine)
            which += jnp.where(mine, ids + 1.0, 0.0)
        blocks = stack_rows(ranks(came), slots)
        label = [
            jnp.sum(jnp.where(block, which[q : q + 1, :], 0.0), axis=1, keepdims=True)
            for q, block in enumerate(blocks)
        ]
        return jnp.concatenate(label, axis=0) - 1.0

    def compute(g, send, midway=None):
        label = labels(g)
        total(drecv.at[g], got.at[g, others])
        x = got[g].reshape(rows, width)
        hidden = []
        for e in range(local):
            gate_val = jnp.dot(x, gate[e], preferred_element_type=f32)
            up_val = jnp.dot(x, up[e], preferred_element_type=f32)
            value = gate_val / (1.0 + jnp.exp(-gate_val)) * up_val
            hidden.append(jnp.where(label == float(e), value, 0.0).astype(bf16))
        for c in range(CHUNKS):
            columns = pl.ds(c * chunk, chunk)
            value = jnp.zeros((rows, chunk), f32)
            for e in range(local):
                value += jnp.dot(hidden[e], down[e, :, columns], preferred_element_type=f32)
            got[g, :, :, columns] = value.astype(bf16).reshape(plane, slots, chunk)
            if send:
                give_back(g, c)
            if midway is not None and c == EARLY - 1:
                midway()

        back[g, p] = got[g, p]

    def shared_hidden(g):
        pre = jnp.dot(
            held[g], spread[:, :, :, :, : 2 * part].reshape(width, 2 * part),
            preferred_element_type=f32,
        )
        gate_val, up_val = pre[:, :part], pre[:, part:]
        hidden_s[g] = (gate_val / (1.0 + jnp.exp(-gate_val)) * up_val).astype(bf16)

    def returned(g, c):
        total(brecv.at[g, c], back.at[g, others, :, pl.ds(c * chunk, chunk)])

    def combined(g, h):
        columns = pl.ds(h * piece, piece)
        value = sum(
            lax.dot_general(
                unpack[g, i], back[g, :, :, columns].reshape(rows, piece),
                (((0,), (0,)), ((), ())), preferred_element_type=f32,
            )
            for i in range(2)
        )
        down_t = spread[:, :, :, :, 2 * part :].reshape(width, part)[h * piece :][:piece]
        return value + lax.dot_general(
            hidden_s[g], down_t, (((1,), (1,)), ((), ())), preferred_element_type=f32
        )

    def land_copy(slot, goal, g, h):
        columns = pl.ds(h * piece, piece)
        return pltpu.make_async_remote_copy(
            src_ref=partial.at[g, :, columns], dst_ref=land.at[slot, :, columns],
            send_sem=lsend.at[0], recv_sem=lrecv.at[slot, h],
            device_id=(goal * plane + p,), device_id_type=MESH,
        )

    def pass_on(k, c, joined=False):
        g = pick(BACK, z, k)
        slot, goal = pick(SLOT, z, k), pick(GOAL, z, k)
        returned(g, c)
        for h in range(c * HALVES, (c + 1) * HALVES):
            columns = pl.ds(h * piece, piece)
            value = combined(g, h)
            if joined:
                extra = k + 1
                land_copy(jnp.int32(extra), goal, g, h).wait_recv()
                value += land[extra, :, columns].astype(f32)
            partial[g, :, columns] = value.astype(bf16)
            land_copy(slot, goal, g, h).start()

    for j in range(1, GROUPS):
        route_copy(j, route.at[p, z], 0).start()
        route_copy(j, share_of.at[z], 1).start()
    for c in range(CHUNKS):

        @pl.when(has_low)
        def _():
            along(z, c, 0).start()

        @pl.when(has_high)
        def _():
            along(z, c, 1).start()

    for j in range(1, GROUPS):
        slice_copy(j).start()
    for goal in near:
        column_copy(goal, z, chip, 0).start()
    make_pack(z)
    for c in range(CHUNKS):
        fill(z, c)
        dispatch(z, c)
    total(rrecv.at[0], route.at[p, pl.ds(0, GROUPS - 1)])
    total(rrecv.at[1], share_of.at[pl.ds(0, GROUPS - 1)])
    for i in range(1, plane):
        route_forward(i, p).start()
    for j in range(1, GROUPS):
        make_pack((z + j) % GROUPS)

    one, two, three = (pick(ORDER, z, k) for k in range(1, GROUPS))
    for c in range(CHUNKS):
        arrive_chunk(one, c)

        @pl.when(middle)
        def _():
            arrive_chunk(three, c)

        fill(one, c)
        dispatch(one, c)

    total(hzrecv.at[0], spread.at[pl.ds(0, GROUPS - 1), chip, core])
    for goal in near:
        for j in range(1, GROUPS):
            column_copy(goal, (z + j) % GROUPS, chip, 0).start()
    total(frecv.at[0], route.at[others])
    for copy in weights:
        copy.wait()
    compute(z, False)

    def hand_over():
        total(hprecv.at[0], spread.at[:, pl.ds(0, len(near)), core])
        if square:
            for g in range(GROUPS // 2):
                column_copy(across, g, beside, 1).start()
            for g in range(GROUPS // 2, GROUPS):
                column_copy(beside, g, across, 1).start()

    def share():
        if square:
            total(hprecv.at[1], spread.at[:, 0, core])
        core_copy(core).start()

    for c in range(CHUNKS):
        arrive_chunk(two, c)
        fill(two, c)
        dispatch(two, c)
        if c == 1:

            @pl.when(middle)
            def _():
                hand_over()

    @pl.when(outer)
    def _():
        hand_over()

    compute(one, False)

    @pl.when(outer)
    def _():
        for c in range(EARLY):
            give_back(one, c)
        for c in range(EARLY):
            arrive_chunk(three, c)
            fill(three, c)
            dispatch(three, c)
        share()

    @pl.when(middle)
    def _():
        fill(three, 0)
        dispatch(three, 0)

    def rest_of_three():
        @pl.when(outer)
        def _():
            for c in range(EARLY, CHUNKS):
                arrive_chunk(three, c)
                fill(three, c)
                dispatch(three, c)

    compute(two, True, rest_of_three)

    @pl.when(outer)
    def _():
        core_copy(1 - core).wait_recv()
        shared_hidden(one)
        for c in range(EARLY):
            pass_on(0, c)
        shared_hidden(two)
        for c in range(EARLY):
            pass_on(1, c)

    @pl.when(middle)
    def _():
        for c in range(EARLY):
            give_back(one, c)
        for c in range(1, CHUNKS):
            fill(three, c)
            dispatch(three, c)
        for c in range(EARLY, CHUNKS):
            give_back(one, c)
        share()
        core_copy(1 - core).wait_recv()
        shared_hidden(two)
        for c in range(CHUNKS):
            pass_on(0, c)
        shared_hidden(one)
        for c in range(EARLY):
            pass_on(1, c, True)

    def third_of_two():
        @pl.when(outer)
        def _():
            pass_on(1, EARLY)

    compute(three, True, third_of_two)

    @pl.when(outer)
    def _():
        for c in range(EARLY, CHUNKS):
            give_back(one, c)

    for c in range(CHUNKS):
        give_back(z, c)

    @pl.when(outer)
    def _():
        shared_hidden(three)
        for c in range(EARLY + 1, CHUNKS):
            pass_on(1, c)
        for c in range(CHUNKS):
            pass_on(2, c)
        for c in range(EARLY, CHUNKS):
            pass_on(0, c)

    @pl.when(middle)
    def _():
        shared_hidden(three)
        for c in range(EARLY, CHUNKS):
            pass_on(1, c, True)
        for c in range(CHUNKS):
            pass_on(2, c, True)

    shared_hidden(z)
    for c in range(CHUNKS):
        returned(z, c)
        for h in range(c * HALVES, (c + 1) * HALVES):
            columns = pl.ds(h * piece, piece)
            value = combined(z, h)
            for slot in range(2):
                land_copy(jnp.int32(slot), z, z, h).wait_recv()
                value += land[slot, :, columns].astype(f32)
            out_ref[:, columns] = value.astype(out_ref.dtype)

    total(rsend.at[0], route.at[p, pl.ds(0, GROUPS - 1)])
    total(rsend.at[1], share_of.at[pl.ds(0, GROUPS - 1)])
    total(hzsend.at[0], slices.at[pl.ds(0, GROUPS - 1)])
    total(fsend.at[0], route.at[others])
    total(hpsend.at[0], spread.at[:, pl.ds(0, chips - 1), core])
    core_copy(core).wait_send()
    total(dsend.at[0], packed.at[:, others])
    total(bsend.at[0], got.at[:, others])
    total(lsend.at[0], partial.at[pl.ds(0, GROUPS - 1)])
    for g in range(GROUPS):

        @pl.when(jnp.logical_and(g >= z, has_low))
        def _():
            total(zsend.at[0, g], held.at[g])

        @pl.when(jnp.logical_and(g <= z, has_high))
        def _():
            total(zsend.at[1, g], held.at[g])


def per_device(
    tokens, norm_gain, expert_ids, gate_weights, expert_gate, expert_up, expert_down,
    shared_gate, shared_up, shared_down,
):
    bf16, f32 = jnp.bfloat16, jnp.float32
    count_tok, width = tokens.shape
    top = expert_ids.shape[1]
    local = expert_gate.shape[0]
    devices = lax.axis_size("ep")
    plane = devices // GROUPS
    mean_rows = count_tok * top // devices
    capacity = mean_rows + mean_rows // 2
    slots = -(-capacity // 8) * 8
    rows = plane * slots
    depth, hidden = shared_gate.shape
    part = hidden // GROUPS
    dma = pltpu.SemaphoreType.DMA
    hbm = pl.BlockSpec(memory_space=pltpu.HBM)
    blocks = (GROUPS, plane, slots, width)
    whole = (GROUPS, count_tok, width)
    return pl.pallas_call(
        functools.partial(moe_kernel, plane, slots, local),
        out_shape=jax.ShapeDtypeStruct((count_tok, width), bf16),
        in_specs=[hbm] * 10,
        out_specs=pl.BlockSpec(memory_space=pltpu.VMEM),
        scratch_shapes=[
            pltpu.VMEM(tokens.shape, bf16),
            pltpu.VMEM((1, width), f32),
            pltpu.VMEM((top, count_tok), jnp.int32),
            pltpu.VMEM((top, count_tok), f32),
            pltpu.VMEM(shared_gate.shape, bf16),
            pltpu.VMEM(shared_gate.shape, bf16),
            pltpu.VMEM(shared_gate.shape, bf16),
            dma((7,)),
            pltpu.VMEM(expert_gate.shape, bf16),
            pltpu.VMEM(expert_up.shape, bf16),
            pltpu.VMEM(expert_down.shape, bf16),
            pltpu.VMEM(whole, bf16),
            pltpu.VMEM((GROUPS, rows, count_tok), bf16),
            pltpu.VMEM((GROUPS, 2, rows, count_tok), bf16),
            pltpu.VMEM(blocks, bf16),
            pltpu.VMEM(blocks, bf16),
            pltpu.VMEM(blocks, bf16),
            pltpu.VMEM(whole, bf16),
            pltpu.VMEM(whole, bf16),
            pltpu.VMEM((plane, GROUPS, top, count_tok), f32),
            pltpu.VMEM((GROUPS, top, count_tok), f32),
            pltpu.VMEM((GROUPS, depth, 3 * part), bf16),
            pltpu.VMEM((GROUPS, plane // 2, 2, depth, 3 * part), bf16),
            pltpu.VMEM((GROUPS, count_tok, part), bf16),
            dma((3,)),
            dma((2,)),
            dma((2,)),
            dma((1,)),
            dma((1,)),
            dma((1,)),
            dma((1,)),
            dma((1,)),
            dma((2,)),
            dma((1,)),
            dma((1,)),
            dma((2, GROUPS)),
            dma((GROUPS, CHUNKS)),
            dma((1,)),
            dma((GROUPS,)),
            dma((1,)),
            dma((GROUPS, CHUNKS)),
            dma((1,)),
            dma((GROUPS, CHUNKS * HALVES)),
        ],
        compiler_params=pltpu.CompilerParams(
            collective_id=0, has_side_effects=True, vmem_limit_bytes=52 * 1024 * 1024
        ),
    )(
        *[
            pltpu.with_memory_space_constraint(x, pltpu.HBM)
            for x in (
                tokens, norm_gain.reshape(1, width), expert_ids.T, gate_weights.T,
                shared_gate, shared_up, shared_down.T, expert_gate, expert_up, expert_down,
            )
        ]
    )


def solution(mesh):
    return jax.shard_map(
        per_device,
        mesh=mesh,
        in_specs=(
            P("ep", None),
            P(),
            P("ep", None),
            P("ep", None),
            P("ep", None, None),
            P("ep", None, None),
            P("ep", None, None),
            P("ep", None),
            P("ep", None),
            P(None, "ep"),
        ),
        out_specs=P("ep", None),
        check_vma=False,
    )
```

```python
import functools

import jax
import jax.numpy as jnp
from jax import lax
from jax.experimental import pallas as pl
from jax.experimental.pallas import tpu as pltpu
from jax.sharding import PartitionSpec as P

EPS = 1e-06
GROUPS = 4
CHUNKS = 4
EARLY = 2
HALVES = 2
MESH = pl.DeviceIdType.MESH
ORDER = ((0, 1, 2, 3), (1, 2, 3, 0), (2, 1, 0, 3), (3, 2, 1, 0))
BACK = ((1, 2, 3), (3, 2, 0), (0, 1, 3), (2, 1, 0))
GOAL = ((1, 1, 2), (3, 2, 0), (0, 1, 3), (2, 2, 1))
SLOT = ((0, 2, 3), (1, 1, 0), (1, 1, 0), (0, 2, 3))


def pick(table, row, column):
    value = jnp.int32(table[0][column])
    for i in range(1, len(table)):
        value = jnp.where(row == i, jnp.int32(table[i][column]), value)
    return value


def stack_rows(rank, slots):
    slot = lax.broadcasted_iota(jnp.int32, (slots, rank.shape[1]), 0).astype(jnp.float32)
    return [rank[q : q + 1, :] == slot for q in range(rank.shape[0])]


def moe_kernel(
    plane, slots, local,
    tok_hbm, gain_hbm, ids_hbm, wts_hbm, sgate_hbm, sup_hbm, sdown_hbm,
    gate_hbm, up_hbm, down_hbm,
    out_ref,
    tok_ref, gain_ref, ids_ref, wts_ref, sgate_ref, sup_ref, sdown_ref, in_sem,
    gate, up, down, held, pack, unpack, packed, got, back, partial, land, route, share_of, slices, spread, hidden_s,
    w_sem, rsend, rrecv, fsend, frecv, hzsend, hzrecv, hpsend, hprecv, hcsend, hcrecv,
    zsend, zrecv, dsend, drecv, bsend, brecv, lsend, lrecv,
):
    f32, bf16 = jnp.float32, jnp.bfloat16
    me = lax.axis_index("ep")
    z, p = me // plane, me % plane
    chips, chip, core = plane // 2, p // 2, p % 2
    has_low, has_high = z > 0, z < GROUPS - 1
    middle = jnp.logical_and(has_low, has_high)
    outer = jnp.logical_not(middle)
    count_tok, width = tok_ref.shape
    top = ids_ref.shape[0]
    rows = plane * slots
    part = sgate_ref.shape[1] // GROUPS
    chunk = width // CHUNKS
    piece = chunk // HALVES

    inputs = [
        pltpu.make_async_copy(src, dst, in_sem.at[i])
        for i, (src, dst) in enumerate(
            (
                (tok_hbm, tok_ref), (gain_hbm, gain_ref), (ids_hbm, ids_ref),
                (wts_hbm, wts_ref), (sgate_hbm, sgate_ref), (sup_hbm, sup_ref),
                (sdown_hbm, sdown_ref),
            )
        )
    ]
    for copy in inputs:
        copy.start()
    barrier = pltpu.get_barrier_semaphore()

    def greet(device):
        pl.semaphore_signal(barrier, inc=1, device_id=(device,), device_id_type=MESH)

    for i in range(1, plane):
        greet(z * plane + (p + i) % plane)
    for j in range(1, GROUPS):
        greet((z + j) % GROUPS * plane + p)

    weights = [
        pltpu.make_async_copy(src, dst, w_sem.at[i])
        for i, (src, dst) in enumerate(((gate_hbm, gate), (up_hbm, up), (down_hbm, down)))
    ]
    for copy in weights:
        copy.start()

    for copy in inputs:
        copy.wait()
    for g in range(GROUPS):
        for i, ref in enumerate((sgate_ref, sup_ref, sdown_ref)):
            slices[g, :, i * part : (i + 1) * part] = ref[:, g * part : (g + 1) * part]
    route[p, z] = ids_ref[...].astype(f32)
    share_of[z] = wts_ref[...]
    values = tok_ref[...].astype(f32)
    scaled = values * lax.rsqrt(jnp.mean(values * values, axis=-1, keepdims=True) + EPS)
    held[z] = (scaled * gain_ref[...]).astype(bf16)
    spread[z, chip, core] = slices[z]

    before = (
        lax.broadcasted_iota(jnp.int32, (count_tok, count_tok), 0)
        < lax.broadcasted_iota(jnp.int32, (count_tok, count_tok), 1)
    ).astype(bf16)

    def ranks(named):
        rank = jnp.dot(named.astype(bf16), before, preferred_element_type=f32)
        return jnp.where(named, rank, -1.0)

    def make_pack(g):
        first = (
            (lax.broadcasted_iota(jnp.int32, (plane, count_tok), 0) + z * plane) * local
        ).astype(f32)
        named = jnp.zeros((plane, count_tok), jnp.bool_)
        scale = jnp.zeros((plane, count_tok), f32)
        for k in range(top):
            ids = route[p, g, k : k + 1, :]
            here = jnp.logical_and(ids >= first, ids < first + float(local))
            named = jnp.logical_or(named, here)
            scale += jnp.where(here, share_of[g, k : k + 1, :], 0.0)
        blocks = stack_rows(ranks(named), slots)
        pack[g] = jnp.concatenate([b.astype(f32) for b in blocks], axis=0).astype(bf16)
        weighted = jnp.concatenate(
            [jnp.where(b, scale[q : q + 1, :], 0.0) for q, b in enumerate(blocks)], axis=0
        )
        upper = weighted.astype(bf16)
        unpack[g, 0] = upper
        unpack[g, 1] = (weighted - upper.astype(f32)).astype(bf16)

    def fill(g, c):
        columns = pl.ds(c * chunk, chunk)
        packed[g, :, :, columns] = (
            jnp.dot(pack[g], held[g, :, columns], preferred_element_type=f32)
            .astype(bf16)
            .reshape(plane, slots, chunk)
        )

    pl.semaphore_wait(barrier, plane - 1 + GROUPS - 1)

    def total(sem, block):
        return pltpu.make_async_copy(block, block, sem).wait()

    others = pl.ds(0, plane - 1)

    def route_copy(j, ref, sem):
        return pltpu.make_async_remote_copy(
            src_ref=ref, dst_ref=ref,
            send_sem=rsend.at[sem], recv_sem=rrecv.at[sem],
            device_id=((z + j) % GROUPS * plane + p,), device_id_type=MESH,
        )

    def route_forward(i, q):
        return pltpu.make_async_remote_copy(
            src_ref=route.at[q], dst_ref=route.at[q],
            send_sem=fsend.at[0], recv_sem=frecv.at[0],
            device_id=(z * plane + (p + i) % plane,), device_id_type=MESH,
        )

    def slice_copy(j):
        g = (z + j) % GROUPS
        return pltpu.make_async_remote_copy(
            src_ref=slices.at[g], dst_ref=spread.at[z, chip, core],
            send_sem=hzsend.at[0], recv_sem=hzrecv.at[0],
            device_id=(g * plane + p,), device_id_type=MESH,
        )

    def column_copy(goal, g, c, sem):
        return pltpu.make_async_remote_copy(
            src_ref=spread.at[g, c, core], dst_ref=spread.at[g, c, core],
            send_sem=hpsend.at[0], recv_sem=hprecv.at[sem],
            device_id=(z * plane + goal * 2 + core,), device_id_type=MESH,
        )

    square = chips == 4
    beside, across = chip + 1 - 2 * (chip % 2), (chip + 2) % chips
    near = (beside, across) if square else [(chip + i) % chips for i in range(1, chips)]

    def core_copy(c):
        return pltpu.make_async_remote_copy(
            src_ref=spread.at[:, :, c], dst_ref=spread.at[:, :, c],
            send_sem=hcsend.at[0], recv_sem=hcrecv.at[0],
            device_id=(me + 1 - 2 * core,), device_id_type=MESH,
        )

    def along(g, c, direction):
        block = held.at[g, :, pl.ds(c * chunk, chunk)]
        return pltpu.make_async_remote_copy(
            src_ref=block, dst_ref=block,
            send_sem=zsend.at[direction, g], recv_sem=zrecv.at[g, c],
            device_id=(me + (plane if direction else -plane),), device_id_type=MESH,
        )

    def arrive_chunk(g, c):
        along(g, c, 0).wait_recv()

        @pl.when(jnp.logical_and(g > z, has_low))
        def _():
            along(g, c, 0).start()

        @pl.when(jnp.logical_and(g < z, has_high))
        def _():
            along(g, c, 1).start()

    def arrive(g):
        for c in range(CHUNKS):
            arrive_chunk(g, c)

    def dispatch_copy(g, q, c):
        columns = pl.ds(c * chunk, chunk)
        return pltpu.make_async_remote_copy(
            src_ref=packed.at[g, q, :, columns], dst_ref=got.at[g, p, :, columns],
            send_sem=dsend.at[0], recv_sem=drecv.at[g],
            device_id=(z * plane + q,), device_id_type=MESH,
        )

    def return_copy(g, q, c):
        columns = pl.ds(c * chunk, chunk)
        return pltpu.make_async_remote_copy(
            src_ref=got.at[g, q, :, columns], dst_ref=back.at[g, p, :, columns],
            send_sem=bsend.at[0], recv_sem=brecv.at[g, c],
            device_id=(z * plane + q,), device_id_type=MESH,
        )

    def dispatch(g, c):
        for i in range(1, plane):
            dispatch_copy(g, (p + i) % plane, c).start()
        columns = pl.ds(c * chunk, chunk)
        got[g, p, :, columns] = packed[g, p, :, columns]

    def give_back(g, c):
        for i in range(1, plane):
            return_copy(g, (p + i) % plane, c).start()

    def labels(g):
        came = jnp.zeros((plane, count_tok), jnp.bool_)
        which = jnp.zeros((plane, count_tok), f32)
        first = (me * local).astype(f32)
        for k in range(top):
            ids = route[:, g, k, :] - first
            mine = jnp.logical_and(ids >= 0.0, ids < float(local))
            came = jnp.logical_or(came, mine)
            which += jnp.where(mine, ids + 1.0, 0.0)
        blocks = stack_rows(ranks(came), slots)
        label = [
            jnp.sum(jnp.where(block, which[q : q + 1, :], 0.0), axis=1, keepdims=True)
            for q, block in enumerate(blocks)
        ]
        return jnp.concatenate(label, axis=0) - 1.0

    def compute(g, send, midway=None):
        label = labels(g)
        total(drecv.at[g], got.at[g, others])
        x = got[g].reshape(rows, width)
        hidden = []
        for e in range(local):
            gate_val = jnp.dot(x, gate[e], preferred_element_type=f32)
            up_val = jnp.dot(x, up[e], preferred_element_type=f32)
            value = gate_val / (1.0 + jnp.exp(-gate_val)) * up_val
            hidden.append(jnp.where(label == float(e), value, 0.0).astype(bf16))
        for c in range(CHUNKS):
            columns = pl.ds(c * chunk, chunk)
            value = jnp.zeros((rows, chunk), f32)
            for e in range(local):
                value += jnp.dot(hidden[e], down[e, :, columns], preferred_element_type=f32)
            got[g, :, :, columns] = value.astype(bf16).reshape(plane, slots, chunk)
            if send:
                give_back(g, c)
            if midway is not None and c == EARLY - 1:
                midway()

        back[g, p] = got[g, p]

    def shared_hidden(g):
        pre = jnp.dot(
            held[g], spread[:, :, :, :, : 2 * part].reshape(width, 2 * part),
            preferred_element_type=f32,
        )
        gate_val, up_val = pre[:, :part], pre[:, part:]
        hidden_s[g] = (gate_val / (1.0 + jnp.exp(-gate_val)) * up_val).astype(bf16)

    def returned(g, c):
        total(brecv.at[g, c], back.at[g, others, :, pl.ds(c * chunk, chunk)])

    def combined(g, h):
        columns = pl.ds(h * piece, piece)
        value = sum(
            lax.dot_general(
                unpack[g, i], back[g, :, :, columns].reshape(rows, piece),
                (((0,), (0,)), ((), ())), preferred_element_type=f32,
            )
            for i in range(2)
        )
        down_t = spread[:, :, :, :, 2 * part :].reshape(width, part)[h * piece :][:piece]
        return value + lax.dot_general(
            hidden_s[g], down_t, (((1,), (1,)), ((), ())), preferred_element_type=f32
        )

    def land_copy(slot, goal, g, h):
        columns = pl.ds(h * piece, piece)
        return pltpu.make_async_remote_copy(
            src_ref=partial.at[g, :, columns], dst_ref=land.at[slot, :, columns],
            send_sem=lsend.at[0], recv_sem=lrecv.at[slot, h],
            device_id=(goal * plane + p,), device_id_type=MESH,
        )

    def pass_on(k, c, joined=False):
        g = pick(BACK, z, k)
        slot, goal = pick(SLOT, z, k), pick(GOAL, z, k)
        returned(g, c)
        for h in range(c * HALVES, (c + 1) * HALVES):
            columns = pl.ds(h * piece, piece)
            value = combined(g, h)
            if joined:
                extra = k + 1
                land_copy(jnp.int32(extra), goal, g, h).wait_recv()
                value += land[extra, :, columns].astype(f32)
            partial[g, :, columns] = value.astype(bf16)
            land_copy(slot, goal, g, h).start()

    for j in range(1, GROUPS):
        route_copy(j, route.at[p, z], 0).start()
        route_copy(j, share_of.at[z], 1).start()
    for c in range(CHUNKS):

        @pl.when(has_low)
        def _():
            along(z, c, 0).start()

        @pl.when(has_high)
        def _():
            along(z, c, 1).start()

    for j in range(1, GROUPS):
        slice_copy(j).start()
    for goal in near:
        column_copy(goal, z, chip, 0).start()
    make_pack(z)
    for c in range(CHUNKS):
        fill(z, c)
        dispatch(z, c)
    total(rrecv.at[0], route.at[p, pl.ds(0, GROUPS - 1)])
    total(rrecv.at[1], share_of.at[pl.ds(0, GROUPS - 1)])
    for i in range(1, plane):
        route_forward(i, p).start()
    for j in range(1, GROUPS):
        make_pack((z + j) % GROUPS)

    one, two, three = (pick(ORDER, z, k) for k in range(1, GROUPS))
    for c in range(CHUNKS):
        arrive_chunk(one, c)

        @pl.when(middle)
        def _():
            arrive_chunk(three, c)

        fill(one, c)
        dispatch(one, c)

    total(hzrecv.at[0], spread.at[pl.ds(0, GROUPS - 1), chip, core])
    for goal in near:
        for j in range(1, GROUPS):
            column_copy(goal, (z + j) % GROUPS, chip, 0).start()
    total(frecv.at[0], route.at[others])
    for copy in weights:
        copy.wait()
    compute(z, False)

    def hand_over():
        total(hprecv.at[0], spread.at[:, pl.ds(0, len(near)), core])
        if square:
            for g in range(GROUPS // 2):
                column_copy(across, g, beside, 1).start()
            for g in range(GROUPS // 2, GROUPS):
                column_copy(beside, g, across, 1).start()

    def share():
        if square:
            total(hprecv.at[1], spread.at[:, 0, core])
        core_copy(core).start()

    for c in range(CHUNKS):
        arrive_chunk(two, c)
        fill(two, c)
        dispatch(two, c)
        if c == 1:

            @pl.when(middle)
            def _():
                hand_over()

    @pl.when(outer)
    def _():
        hand_over()

    compute(one, False)

    @pl.when(outer)
    def _():
        for c in range(EARLY):
            give_back(one, c)
        for c in range(EARLY):
            arrive_chunk(three, c)
            fill(three, c)
            dispatch(three, c)
        share()

    @pl.when(middle)
    def _():
        fill(three, 0)
        dispatch(three, 0)

    def rest_of_three():
        @pl.when(outer)
        def _():
            for c in range(EARLY, CHUNKS):
                arrive_chunk(three, c)
                fill(three, c)
                dispatch(three, c)

    compute(two, True, rest_of_three)

    @pl.when(outer)
    def _():
        core_copy(1 - core).wait_recv()
        shared_hidden(one)
        for c in range(EARLY):
            pass_on(0, c)
        shared_hidden(two)
        for c in range(EARLY):
            pass_on(1, c)

    @pl.when(middle)
    def _():
        for c in range(EARLY):
            give_back(one, c)
        for c in range(1, CHUNKS):
            fill(three, c)
            dispatch(three, c)
        for c in range(EARLY, CHUNKS):
            give_back(one, c)
        share()
        core_copy(1 - core).wait_recv()
        shared_hidden(two)
        for c in range(CHUNKS):
            pass_on(0, c)
        shared_hidden(one)
        for c in range(EARLY):
            pass_on(1, c, True)

    def third_of_two():
        @pl.when(outer)
        def _():
            pass_on(1, EARLY)

    compute(three, True, third_of_two)

    @pl.when(outer)
    def _():
        for c in range(EARLY, CHUNKS):
            give_back(one, c)

    for c in range(CHUNKS):
        give_back(z, c)

    @pl.when(outer)
    def _():
        shared_hidden(three)
        for c in range(CHUNKS):
            pass_on(2, c)
        for c in range(EARLY + 1, CHUNKS):
            pass_on(1, c)
        for c in range(EARLY, CHUNKS):
            pass_on(0, c)

    @pl.when(middle)
    def _():
        shared_hidden(three)
        pass_on(1, EARLY, True)
        for c in range(CHUNKS):
            pass_on(2, c, True)
        for c in range(EARLY + 1, CHUNKS):
            pass_on(1, c, True)

    shared_hidden(z)
    for c in range(CHUNKS):
        returned(z, c)
        for h in range(c * HALVES, (c + 1) * HALVES):
            columns = pl.ds(h * piece, piece)
            value = combined(z, h)
            for slot in range(2):
                land_copy(jnp.int32(slot), z, z, h).wait_recv()
                value += land[slot, :, columns].astype(f32)
            out_ref[:, columns] = value.astype(out_ref.dtype)

    total(rsend.at[0], route.at[p, pl.ds(0, GROUPS - 1)])
    total(rsend.at[1], share_of.at[pl.ds(0, GROUPS - 1)])
    total(hzsend.at[0], slices.at[pl.ds(0, GROUPS - 1)])
    total(fsend.at[0], route.at[others])
    total(hpsend.at[0], spread.at[:, pl.ds(0, chips - 1), core])
    core_copy(core).wait_send()
    total(dsend.at[0], packed.at[:, others])
    total(bsend.at[0], got.at[:, others])
    total(lsend.at[0], partial.at[pl.ds(0, GROUPS - 1)])
    for g in range(GROUPS):

        @pl.when(jnp.logical_and(g >= z, has_low))
        def _():
            total(zsend.at[0, g], held.at[g])

        @pl.when(jnp.logical_and(g <= z, has_high))
        def _():
            total(zsend.at[1, g], held.at[g])


def per_device(
    tokens, norm_gain, expert_ids, gate_weights, expert_gate, expert_up, expert_down,
    shared_gate, shared_up, shared_down,
):
    bf16, f32 = jnp.bfloat16, jnp.float32
    count_tok, width = tokens.shape
    top = expert_ids.shape[1]
    local = expert_gate.shape[0]
    devices = lax.axis_size("ep")
    plane = devices // GROUPS
    mean_rows = count_tok * top // devices
    capacity = mean_rows + mean_rows // 2
    slots = -(-capacity // 8) * 8
    rows = plane * slots
    depth, hidden = shared_gate.shape
    part = hidden // GROUPS
    dma = pltpu.SemaphoreType.DMA
    hbm = pl.BlockSpec(memory_space=pltpu.HBM)
    blocks = (GROUPS, plane, slots, width)
    whole = (GROUPS, count_tok, width)
    return pl.pallas_call(
        functools.partial(moe_kernel, plane, slots, local),
        out_shape=jax.ShapeDtypeStruct((count_tok, width), bf16),
        in_specs=[hbm] * 10,
        out_specs=pl.BlockSpec(memory_space=pltpu.VMEM),
        scratch_shapes=[
            pltpu.VMEM(tokens.shape, bf16),
            pltpu.VMEM((1, width), f32),
            pltpu.VMEM((top, count_tok), jnp.int32),
            pltpu.VMEM((top, count_tok), f32),
            pltpu.VMEM(shared_gate.shape, bf16),
            pltpu.VMEM(shared_gate.shape, bf16),
            pltpu.VMEM(shared_gate.shape, bf16),
            dma((7,)),
            pltpu.VMEM(expert_gate.shape, bf16),
            pltpu.VMEM(expert_up.shape, bf16),
            pltpu.VMEM(expert_down.shape, bf16),
            pltpu.VMEM(whole, bf16),
            pltpu.VMEM((GROUPS, rows, count_tok), bf16),
            pltpu.VMEM((GROUPS, 2, rows, count_tok), bf16),
            pltpu.VMEM(blocks, bf16),
            pltpu.VMEM(blocks, bf16),
            pltpu.VMEM(blocks, bf16),
            pltpu.VMEM(whole, bf16),
            pltpu.VMEM(whole, bf16),
            pltpu.VMEM((plane, GROUPS, top, count_tok), f32),
            pltpu.VMEM((GROUPS, top, count_tok), f32),
            pltpu.VMEM((GROUPS, depth, 3 * part), bf16),
            pltpu.VMEM((GROUPS, plane // 2, 2, depth, 3 * part), bf16),
            pltpu.VMEM((GROUPS, count_tok, part), bf16),
            dma((3,)),
            dma((2,)),
            dma((2,)),
            dma((1,)),
            dma((1,)),
            dma((1,)),
            dma((1,)),
            dma((1,)),
            dma((2,)),
            dma((1,)),
            dma((1,)),
            dma((2, GROUPS)),
            dma((GROUPS, CHUNKS)),
            dma((1,)),
            dma((GROUPS,)),
            dma((1,)),
            dma((GROUPS, CHUNKS)),
            dma((1,)),
            dma((GROUPS, CHUNKS * HALVES)),
        ],
        compiler_params=pltpu.CompilerParams(
            collective_id=0, has_side_effects=True, vmem_limit_bytes=52 * 1024 * 1024
        ),
    )(
        *[
            pltpu.with_memory_space_constraint(x, pltpu.HBM)
            for x in (
                tokens, norm_gain.reshape(1, width), expert_ids.T, gate_weights.T,
                shared_gate, shared_up, shared_down.T, expert_gate, expert_up, expert_down,
            )
        ]
    )


def solution(mesh):
    return jax.shard_map(
        per_device,
        mesh=mesh,
        in_specs=(
            P("ep", None),
            P(),
            P("ep", None),
            P("ep", None),
            P("ep", None, None),
            P("ep", None, None),
            P("ep", None, None),
            P("ep", None),
            P("ep", None),
            P(None, "ep"),
        ),
        out_specs=P("ep", None),
        check_vma=False,
    )
```
